512 devices in a mesh: sp: 64 (over z, y), tp: 8 (over x, core).
Axes of the slice: x: 4, y: 4, z: 16, core: 2. Of those that a mesh axis runs over, the one named last changes fastest.
Arguments:
- normed: bfloat16 [16384, 2048], P(('sp', 'tp')), may hold values from -40 to 40
- query_weight: bfloat16 [2048, 2048], P(None, 'tp'), may hold values from -1.5 to 1.5
- key_weight: bfloat16 [2048, 2048], P(None, 'tp'), may hold values from -1 to 1
- value_weight: bfloat16 [2048, 2048], P(None, 'tp'), may hold values from -0.125 to 0.125
- pool_in_weight: bfloat16 [2048, 1024], P(None, 'tp'), may hold values from -0.125 to 0.125
- pool_weight: bfloat16 [8, 128, 128], P('tp'), may hold values from -0.5 to 0.5
- map_balance: float32 [8], replicated, may hold values from 0.3 to 0.8
- head_gain: float32 [256], replicated, may hold values from 0.1 to 1.9
- contrast_out_weight: bfloat16 [2048, 2048], P('tp'), may hold values from -0.109375 to 0.109375
- pool_out_weight: bfloat16 [1024, 2048], P('tp'), may hold values from -0.109375 to 0.109375
Outputs:
- layer_out: bfloat16 [16384, 2048], P(('sp', 'tp'))
The draws below stay inside these ranges and needn't reach their ends.
All inputs are finite; a program needn't handle non-finite values.
Results may differ from the reference program's by a relative error of at most 0.03.
Values may be sent and summed in bfloat16 or wider, within the bound.
A program may use at most 128 MiB of HBM per device.

```python
import math
import jax
import jax.numpy as jnp
from jax import lax

D = 2048
HEADS = 8
HEAD_DIM = 128
GROUPS = 8
GROUP_WIDTH = 128
TOKENS = 16384
N_TP = 8


def shared_keys(key):
    gaussian = jnp.clip(jax.random.normal(jax.random.fold_in(key, 11), (D, 2 * HEADS * HEAD_DIM), jnp.float32), -6.0, 6.0)
    return gaussian * (1.3 / math.sqrt(D))


def draw_key_weight(key, part):
    return shared_keys(key).astype(jnp.bfloat16)


def draw_query_weight(key, part):
    independent = jnp.clip(jax.random.normal(jax.random.fold_in(key, 12), (D, 2 * HEADS * HEAD_DIM), jnp.float32), -6.0, 6.0) * (1.3 / math.sqrt(D))
    aligned = independent
    return aligned.astype(jnp.bfloat16)


def draw_normed(key, part):
    gaussian = jax.random.normal(jax.random.fold_in(key, 21), (TOKENS, D), jnp.float32)
    return jnp.clip(gaussian, -6.0, 6.0).astype(jnp.bfloat16)


def level_of(own_key, dims, pieces, smallest, high):
    def one(dim, parts):
        heights = jax.random.uniform(jax.random.fold_in(jax.random.fold_in(own_key, 6), dim), (parts,), jnp.float32, smallest / len(pieces), high / len(pieces))
        return jnp.repeat(jnp.exp(heights), dims[dim] // parts).reshape((-1,) + (1,) * (len(dims) - dim - 1))

    gain = one(*pieces[0])
    for cut in pieces[1:]:
        gain = gain * one(*cut)
    return gain


def noise(own_key, dims, scale, most, shards=(), held_as=jnp.bfloat16):
    array = jax.random.normal(own_key, dims, jnp.float32) * scale
    if len(shards) > 0:
        array = level_of(own_key, dims, shards, -0.22, 0.18) * array
    return jnp.clip(array, min=-most, max=most).astype(held_as)


def setup_inputs(seed: int = 0) -> dict:
    streams_of = jax.random.split(jax.random.key(seed), 11)
    normed = draw_normed(jax.random.fold_in(streams_of[10], 71), 0)
    query_weight = draw_query_weight(jax.random.fold_in(streams_of[10], 71), 0)
    key_weight = draw_key_weight(jax.random.fold_in(streams_of[10], 71), 0)
    value_weight = noise(streams_of[3], (D, 2 * HEADS * HEAD_DIM), D ** -0.5, 0.125, ((1, 8),))
    pool_in_weight = noise(streams_of[4], (D, GROUPS * GROUP_WIDTH), D ** -0.5, 0.125, ((1, 8),))
    pool_weight = noise(streams_of[5], (GROUPS, GROUP_WIDTH, GROUP_WIDTH), GROUP_WIDTH ** -0.5, 0.5, ((0, 8),))
    map_balance = jnp.clip(jax.random.uniform(streams_of[6], (HEADS,), jnp.float32, 0.3, 0.8), 0.3, 0.8)
    head_gain = jnp.clip(1.0 + 0.18 * jax.random.normal(streams_of[7], (2 * HEAD_DIM,), jnp.float32), 0.1, 1.9)
    contrast_out_weight = noise(streams_of[8], (2 * HEADS * HEAD_DIM, D), (2 * HEADS * HEAD_DIM + GROUPS * GROUP_WIDTH) ** -0.5, 0.109375, ((0, 8),))
    pool_out_weight = noise(streams_of[9], (GROUPS * GROUP_WIDTH, D), (2 * HEADS * HEAD_DIM + GROUPS * GROUP_WIDTH) ** -0.5, 0.109375, ((0, 8),))
    return {"normed": normed, "query_weight": query_weight, "key_weight": key_weight, "value_weight": value_weight, "pool_in_weight": pool_in_weight, "pool_weight": pool_weight, "map_balance": map_balance, "head_gain": head_gain, "contrast_out_weight": contrast_out_weight, "pool_out_weight": pool_out_weight}


reach_back = 15
norm_epsilon = 1e-06

def map_output(queries, key_rows, value_rows):
    total_rows = queries.shape[0]
    block_rows = math.gcd(total_rows, 1024)
    score_scale = HEAD_DIM ** (-0.5)
    outputs = []
    for block_index in range(total_rows // block_rows):
        first_row = block_index * block_rows
        last_row = first_row + block_rows
        scores = jnp.dot(queries[first_row:last_row], key_rows[:last_row].T, preferred_element_type=jnp.float32) * score_scale
        query_order = first_row + jnp.arange(block_rows, dtype=jnp.int32)
        key_order = jnp.arange(last_row, dtype=jnp.int32)
        scores = jnp.where(key_order[None, :] <= query_order[:, None], scores, -jnp.inf)
        row_peak = lax.optimization_barrier(jnp.max(scores, axis=1, keepdims=True))
        raised = jnp.exp(scores - row_peak)
        row_total = lax.optimization_barrier(jnp.sum(raised, axis=1, keepdims=True))
        weighted = jnp.dot(raised.astype(jnp.bfloat16), value_rows[:last_row], preferred_element_type=jnp.float32)
        outputs.append((weighted / row_total).astype(jnp.bfloat16))
    return jnp.concatenate(outputs, axis=0)

def reference(normed, query_weight, key_weight, value_weight, pool_in_weight, pool_weight, map_balance, head_gain, contrast_out_weight, pool_out_weight):
    queries = jnp.dot(normed, query_weight, preferred_element_type=jnp.float32).astype(jnp.bfloat16)
    key_rows = jnp.dot(normed, key_weight, preferred_element_type=jnp.float32).astype(jnp.bfloat16)
    value_rows = jnp.dot(normed, value_weight, preferred_element_type=jnp.float32).astype(jnp.bfloat16)
    pool_input = jnp.dot(normed, pool_in_weight, preferred_element_type=jnp.float32).astype(jnp.bfloat16)
    value_width = 2 * HEAD_DIM
    head_outputs = []
    for head in range(HEADS):
        maps = []
        for which in range(2):
            column = (2 * head + which) * HEAD_DIM
            result_map = map_output(queries[:, column:column + HEAD_DIM], key_rows[:, column:column + HEAD_DIM], value_rows[:, head * value_width:(head + 1) * value_width])
            maps.append(lax.optimization_barrier(result_map).astype(jnp.float32))
        contrast = maps[0] - map_balance[head] * maps[1]
        mean_square = lax.optimization_barrier(jnp.mean(contrast * contrast, axis=1, keepdims=True))
        head_outputs.append((contrast * lax.rsqrt(mean_square + norm_epsilon) * head_gain).astype(jnp.bfloat16))
    contrast_out = jnp.concatenate(head_outputs, axis=1)
    total_rows = normed.shape[0]
    pool_width = GROUPS * GROUP_WIDTH
    extended = jnp.concatenate([jnp.zeros((reach_back, pool_width), jnp.float32), pool_input.astype(jnp.float32)], axis=0)
    group_index = jnp.arange(pool_width, dtype=jnp.int32) // GROUP_WIDTH
    widths = jnp.left_shift(jnp.int32(2), group_index % 4)
    window_sum = jnp.zeros((total_rows, pool_width), jnp.float32)
    for offset in range(reach_back + 1):
        window_sum = window_sum + extended[reach_back - offset:reach_back - offset + total_rows] * (offset < widths)[None, :].astype(jnp.float32)
    position = jnp.arange(total_rows, dtype=jnp.int32)
    counts = jnp.minimum(position[:, None] + 1, widths[None, :]).astype(jnp.float32)
    spread = (window_sum / counts - extended[reach_back:]).astype(jnp.bfloat16)
    spread = lax.optimization_barrier(spread).astype(jnp.float32)
    mixed_groups = jnp.einsum('sgc,gce->sge', spread.reshape(total_rows, GROUPS, GROUP_WIDTH), pool_weight.astype(jnp.float32))
    pool_out = mixed_groups.reshape(total_rows, pool_width).astype(jnp.bfloat16)
    diff_rows = 2 * HEADS * HEAD_DIM // N_TP
    pool_rows = GROUPS * GROUP_WIDTH // N_TP
    summed = jnp.zeros((total_rows, D), jnp.float32)
    for part_index in range(N_TP):
        low_diff = part_index * diff_rows
        low_pool = part_index * pool_rows
        partial_value = jnp.dot(contrast_out[:, low_diff:low_diff + diff_rows], contrast_out_weight[low_diff:low_diff + diff_rows], preferred_element_type=jnp.float32)
        partial_value = partial_value + jnp.dot(pool_out[:, low_pool:low_pool + pool_rows], pool_out_weight[low_pool:low_pool + pool_rows], preferred_element_type=jnp.float32)
        summed = summed + lax.optimization_barrier(partial_value.astype(jnp.bfloat16)).astype(jnp.float32)
    return summed.astype(jnp.bfloat16)
```

```python
import functools
import math

import jax
import jax.numpy as jnp
from jax import lax
from jax.experimental import pallas as pl
from jax.experimental.pallas import tpu as pltpu
from jax.sharding import PartitionSpec as P

MESH = pl.DeviceIdType.MESH
F32 = jnp.float32
BF16 = jnp.bfloat16
Y = 4
X = 4
NEG = -1e30
norm_epsilon = 1e-06


def kernel(
    zn,
    normed,
    wq_h,
    wk_h,
    wv_h,
    wp_h,
    pool_weight,
    balance,
    gain,
    cow_h,
    pow_h,
    out,
    xg,
    wq,
    wk,
    wv,
    wp,
    cow,
    pow_,
    q_all,
    k_all,
    v_all,
    acc,
    m_s,
    l_s,
    pin,
    rim,
    ext,
    pool_part,
    ps,
    pst,
    r2,
    r2t,
    rn,
    rnt,
    co,
    part,
    pr,
    xs,
    xr2,
    xrn,
    w_sem,
    xg_send,
    xg_recv,
    up_send,
    dn_send,
    kv_up_recv,
    kv_dn_recv,
    q_send,
    q_recv,
    h_sem,
    ps_send,
    ps_recv,
    pr_send,
    pr_recv,
    xs_send,
    xs_recv,
):
    sp = lax.axis_index("sp")
    tp = lax.axis_index("tp")
    nsp = zn * Y
    z, y = sp // Y, sp % Y
    x, core = tp // 2, tp % 2
    up_hops = zn // 2
    dn_hops = zn // 2 - 1

    def at(zz, yy, xx, cc):
        return {"sp": zz * Y + yy, "tp": xx * 2 + cc}

    partner = at(z, y, x, 1 - core)
    xr, xl = (x + 1) % X, (x + X - 1) % X
    x2 = (x + 2) % X
    yr, yl = (y + 1) % Y, (y + Y - 1) % Y
    y2 = (y + 2) % Y
    zu, zd = (z + 1) % zn, (z + zn - 1) % zn
    x_right, x_left = at(z, y, xr, core), at(z, y, xl, core)
    y_right, y_left = at(z, yr, x, core), at(z, yl, x, core)
    z_up, z_down = at(zu, y, x, core), at(zd, y, x, core)
    next_sp = {"sp": (sp + 1) % nsp, "tp": tp}
    prev_sp = {"sp": (sp + nsp - 1) % nsp, "tp": tp}

    weights = [
        pltpu.make_async_copy(src, dst, w_sem.at[i])
        for i, (src, dst) in enumerate(
            ((wk_h, wk), (wv_h, wv), (wq_h, wq), (wp_h, wp), (pow_h, pow_), (cow_h, cow))
        )
    ]
    for copy in weights:
        copy.start()

    barrier = pltpu.get_barrier_semaphore()
    peers = (partner, x_right, x_left, y_right, y_left, z_up, z_down, next_sp, prev_sp)
    for peer in peers:
        pl.semaphore_signal(barrier, inc=1, device_id=peer, device_id_type=MESH)
    pl.semaphore_wait(barrier, len(peers))

    def remote(src, dst, send, recv, device):
        return pltpu.make_async_remote_copy(
            src_ref=src,
            dst_ref=dst,
            send_sem=send,
            recv_sem=recv,
            device_id=device,
            device_id_type=MESH,
        )

    sent = []

    def send_x(src, slot, half, device):
        copy = remote(src, xg.at[slot, half], xg_send.at[len(sent)], xg_recv.at[slot, half], device)
        copy.start()
        sent.append(copy)

    def got_x(slot, half):
        remote(
            xg.at[slot, half],
            xg.at[slot, half],
            xg_send.at[0],
            xg_recv.at[slot, half],
            partner,
        ).wait_recv()

    def own(half):
        return normed.at[pl.ds(16 * half, 16)]

    send_x(own(0), tp, 0, x_right)
    send_x(own(1), tp, 1, x_left)
    send_x(own(1), tp, 1, x_right)
    send_x(own(0), tp, 0, x_left)
    send_x(own(0), tp, 0, partner)
    send_x(own(1), tp, 1, partner)
    for half in range(2):
        xg[tp, half] = normed[pl.ds(16 * half, 16), :]
    from_left, from_right, from_far = 2 * xl + core, 2 * xr + core, 2 * x2 + core
    got_x(from_left, 0)
    send_x(xg.at[from_left, 0], from_left, 0, x_right)
    got_x(from_right, 1)
    send_x(xg.at[from_right, 1], from_right, 1, x_left)
    send_x(xg.at[from_left, 0], from_left, 0, partner)
    send_x(xg.at[from_right, 1], from_right, 1, partner)
    got_x(from_left, 1)
    send_x(xg.at[from_left, 1], from_left, 1, partner)
    got_x(from_right, 0)
    send_x(xg.at[from_right, 0], from_right, 0, partner)
    got_x(from_far, 0)
    send_x(xg.at[from_far, 0], from_far, 0, partner)
    got_x(from_far, 1)
    send_x(xg.at[from_far, 1], from_far, 1, partner)

    for j in range(Y):
        for c in range(2):
            m_s[j, c] = jnp.full((256, 128), NEG, F32)
            l_s[j, c] = jnp.zeros((256, 128), F32)
            acc[j, c] = jnp.zeros((256, 256), F32)

    for xx in range(X):
        for half in range(2):
            got_x(2 * xx + 1 - core, half)

    def project(weight):
        rows = xg[...].reshape(256, 2048)
        return jnp.dot(rows, weight[...], preferred_element_type=F32).astype(BF16)

    def kv_send(which, slot, hop, up):
        ref = (k_all, v_all)[which]
        sems = up_send if up else dn_send
        recv = kv_up_recv if up else kv_dn_recv
        return remote(
            ref.at[slot],
            ref.at[slot],
            sems.at[hop, which],
            recv.at[slot, which],
            z_up if up else z_down,
        )

    goes_up = z < zn - 1
    goes_down = z < dn_hops

    def kv_first(which):
        @pl.when(goes_up)
        def _():
            kv_send(which, z, 0, True).start()

        @pl.when(goes_down)
        def _():
            kv_send(which, z, 0, False).start()

    weights[0].wait()
    k_all[z] = project(wk)
    kv_first(0)
    weights[1].wait()
    v_all[z] = project(wv)
    kv_first(1)

    q_sent = []

    def send_q(slot, half, device):
        copy = remote(
            q_all.at[slot, half],
            q_all.at[slot, half],
            q_send.at[len(q_sent)],
            q_recv.at[slot, half],
            device,
        )
        copy.start()
        q_sent.append(copy)

    def got_q(slot, half):
        remote(
            q_all.at[slot, half],
            q_all.at[slot, half],
            q_send.at[0],
            q_recv.at[slot, half],
            y_right,
        ).wait_recv()

    weights[2].wait()
    q_all[y] = project(wq).reshape(2, 128, 256)
    send_q(y, 0, y_right)
    send_q(y, 1, y_left)
    send_q(y, 1, y_right)
    send_q(y, 0, y_left)
    weights[3].wait()
    pin[...] = project(wp)
    halo = remote(pin.at[pl.ds(240, 16)], rim, h_sem.at[0], h_sem.at[1], next_sp)
    halo.start()

    factor = 128 ** (-0.5) * math.log2(math.e)

    def attend(j, slot, masked):
        for c in range(2):
            cols = slice(128 * c, 128 * c + 128)
            q = q_all[j].reshape(256, 256)[:, cols]
            k = k_all[slot, :, cols]
            s = lax.dot_general(q, k, (((1,), (1,)), ((), ())), preferred_element_type=F32) * factor
            if masked:
                row = lax.broadcasted_iota(jnp.int32, (256, 256), 0)
                col = lax.broadcasted_iota(jnp.int32, (256, 256), 1)
                s = jnp.where(col <= row, s, NEG)
            before = m_s[j, c]
            peak = jnp.maximum(before, jnp.max(s, axis=1, keepdims=True))
            shrink = jnp.exp2(before - peak)
            p = jnp.exp2(s - jnp.concatenate([peak, peak], axis=1))
            m_s[j, c] = peak
            l_s[j, c] = l_s[j, c] * shrink + jnp.sum(p, axis=1, keepdims=True)
            pv = jnp.dot(p.astype(BF16), v_all[slot], preferred_element_type=F32)
            acc[j, c] = acc[j, c] * jnp.concatenate([shrink, shrink], axis=1) + pv

    def attend_all(slot):
        def body(j, carry):
            attend(j, slot, False)
            return carry

        lax.fori_loop(0, Y, body, 0)

    attend(y, z, True)

    got_q(yl, 0)
    send_q(yl, 0, y_right)
    got_q(yr, 1)
    send_q(yr, 1, y_left)

    halo.wait()
    ext[pl.ds(0, 16), :] = jnp.where(sp > 0, rim[...].astype(F32), 0.0)
    ext[pl.ds(16, 256), :] = pin[...].astype(F32)
    width = jnp.left_shift(jnp.int32(2), tp % 4)
    window = jnp.zeros((256, 128), F32)
    for offset in range(16):
        window = window + jnp.where(offset < width, ext[pl.ds(16 - offset, 256), :], 0.0)
    position = sp * 256 + lax.broadcasted_iota(jnp.int32, (256, 128), 0)
    counts = jnp.minimum(position + 1, width).astype(F32)
    spread = (window / counts - ext[pl.ds(16, 256), :]).astype(BF16)
    pool_out = jnp.dot(spread, pool_weight[0], preferred_element_type=F32).astype(BF16)
    weights[4].wait()
    for n in range(8):
        cols = slice(256 * n, 256 * n + 256)
        pool_part[:, cols] = jnp.dot(pool_out, pow_[:, cols], preferred_element_type=F32)
    weights[5].wait()

    got_q(yl, 1)
    got_q(yr, 0)
    got_q(y2, 0)
    got_q(y2, 1)

    def own_step(j, carry):
        @pl.when(j > y)
        def _():
            attend(j, z, False)

        return carry

    lax.fori_loop(0, Y, own_step, 0)

    def ring_step(s, carry):
        up_block = jnp.maximum(z - s, 0)
        up_here = s <= z
        up_on = jnp.logical_and(up_here, jnp.logical_and(s < up_hops, z < zn - 1))
        dn_block = (z + s) % zn
        dn_here = jnp.logical_and(s <= dn_hops, dn_block < dn_hops)
        dn_on = jnp.logical_and(dn_here, s < dn_hops)
        dn_used = jnp.logical_and(dn_here, z + s >= zn)
        for which in range(2):

            @pl.when(up_here)
            def _():
                kv_send(which, up_block, 0, True).wait_recv()

            @pl.when(up_on)
            def _():
                kv_send(which, up_block, s, True).start()

            @pl.when(dn_here)
            def _():
                kv_send(which, dn_block, 0, False).wait_recv()

            @pl.when(dn_on)
            def _():
                kv_send(which, dn_block, s, False).start()

        @pl.when(up_here)
        def _():
            attend_all(up_block)

        @pl.when(dn_used)
        def _():
            attend_all(dn_block)

        return carry

    lax.fori_loop(1, up_hops + 1, ring_step, 0)

    def state(j, half):
        rows = pl.ds(128 * half, 128)
        return [(m_s[j, c, rows, :], l_s[j, c, rows, :], acc[j, c, rows, :]) for c in range(2)]

    def arrived(payload, stats):
        columns = jnp.concatenate([stats[...], jnp.zeros((120, 128), F32)], axis=0).T
        return [
            (
                jnp.broadcast_to(columns[:, 2 * c : 2 * c + 1], (128, 128)),
                jnp.broadcast_to(columns[:, 2 * c + 1 : 2 * c + 2], (128, 128)),
                payload[:, 256 * c : 256 * c + 256].astype(F32),
            )
            for c in range(2)
        ]

    def joined(first, second):
        result = []
        for (m1, l1, a1), (m2, l2, a2) in zip(first, second):
            peak = jnp.maximum(m1, m2)
            s1, s2 = jnp.exp2(m1 - peak), jnp.exp2(m2 - peak)
            wide1 = jnp.concatenate([s1, s1], axis=1)
            wide2 = jnp.concatenate([s2, s2], axis=1)
            result.append((peak, l1 * s1 + l2 * s2, a1 * wide1 + a2 * wide2))
        return result

    y_sent = []

    def send_state(values, index, payload, stats, device):
        (m0, l0, a0), (m1, l1, a1) = values
        lane = lax.broadcasted_iota(jnp.int32, (128, 128), 1)
        table = jnp.where(lane == 0, m0, jnp.where(lane == 1, l0, jnp.where(lane == 2, m1, l1)))
        pst[index] = table.T[:8]
        ps[index, :, :256] = a0.astype(BF16)
        ps[index, :, 256:] = a1.astype(BF16)
        for i, (src, dst) in enumerate(((ps, payload), (pst, stats))):
            copy = remote(src.at[index], dst, ps_send.at[index, i], ps_recv.at[index, i], device)
            copy.start()
            y_sent.append(copy)

    def got_state(index, payload, stats):
        for i, (src, dst) in enumerate(((ps, payload), (pst, stats))):
            remote(
                src.at[index], dst, ps_send.at[index, i], ps_recv.at[index, i], y_right
            ).wait_recv()

    send_state(state(y2, 0), 0, r2.at[0], r2t.at[0], y_right)
    send_state(state(y2, 1), 1, r2.at[1], r2t.at[1], y_left)
    send_state(state(yr, 1), 2, rn.at[0, 1], rnt.at[0, 1], y_right)
    send_state(state(yl, 0), 3, rn.at[1, 0], rnt.at[1, 0], y_left)
    got_state(0, r2.at[0], r2t.at[0])
    send_state(
        joined(state(yr, 0), arrived(r2.at[0], r2t.at[0])), 4, rn.at[0, 0], rnt.at[0, 0], y_right
    )
    got_state(1, r2.at[1], r2t.at[1])
    send_state(
        joined(state(yl, 1), arrived(r2.at[1], r2t.at[1])), 5, rn.at[1, 1], rnt.at[1, 1], y_left
    )
    level = balance[tp]
    got_state(2, rn.at[0, 1], rnt.at[0, 1])
    got_state(3, rn.at[1, 0], rnt.at[1, 0])
    for half in range(2):
        if half == 0:
            got_state(4, rn.at[0, 0], rnt.at[0, 0])
        else:
            got_state(5, rn.at[1, 1], rnt.at[1, 1])
        whole = state(y, half)
        for side in range(2):
            whole = joined(whole, arrived(rn.at[side, half], rnt.at[side, half]))
        maps = [
            (a / jnp.concatenate([l, l], axis=1)).astype(BF16).astype(F32) for _, l, a in whole
        ]
        contrast = maps[0] - level * maps[1]
        square = jnp.mean(contrast * contrast, axis=1, keepdims=True)
        contrast = contrast * lax.rsqrt(square + norm_epsilon) * gain[...]
        co[pl.ds(128 * half, 128), :] = contrast.astype(BF16)

    mixed = co[...]
    for n in range(8):
        cols = slice(256 * n, 256 * n + 256)
        tile = jnp.dot(mixed, cow[:, cols], preferred_element_type=F32) + pool_part[:, cols]
        part[:, :, :, :, cols] = tile.astype(BF16).reshape(X, 2, 2, 16, 256)
    pair = [
        remote(part.at[xx, 1 - core], pr.at[xx], pr_send.at[xx], pr_recv.at[xx], partner)
        for xx in range(X)
    ]
    for copy in pair:
        copy.start()
    for copy in pair:
        copy.wait_recv()

    def both(owner, half):
        return part[owner, core, half].astype(F32) + pr[owner, half].astype(F32)

    x_sent = []

    def send_sum(value, index, dst, device):
        xs[index] = value.astype(BF16)
        copy = remote(xs.at[index], dst, xs_send.at[index], xs_recv.at[index], device)
        copy.start()
        x_sent.append(copy)

    def got_sum(index, dst):
        remote(xs.at[index], dst, xs_send.at[index], xs_recv.at[index], x_right).wait_recv()

    send_sum(both(x2, 0), 0, xr2.at[0], x_right)
    send_sum(both(x2, 1), 1, xr2.at[1], x_left)
    send_sum(both(xr, 1), 2, xrn.at[0, 1], x_right)
    send_sum(both(xl, 0), 3, xrn.at[1, 0], x_left)
    got_sum(0, xr2.at[0])
    send_sum(both(xr, 0) + xr2[0].astype(F32), 4, xrn.at[0, 0], x_right)
    got_sum(1, xr2.at[1])
    send_sum(both(xl, 1) + xr2[1].astype(F32), 5, xrn.at[1, 1], x_left)
    got_sum(2, xrn.at[0, 1])
    got_sum(3, xrn.at[1, 0])
    got_sum(4, xrn.at[0, 0])
    got_sum(5, xrn.at[1, 1])
    for half in range(2):
        total = both(x, half) + xrn[0, half].astype(F32) + xrn[1, half].astype(F32)
        out[pl.ds(16 * half, 16), :] = total.astype(BF16)

    for copy in sent + q_sent + y_sent + pair + x_sent:
        copy.wait_send()

    def drain(s, carry):
        up_on = jnp.logical_and(s <= z, goes_up)
        dn_on = (z + s) % zn < dn_hops
        for which in range(2):

            @pl.when(up_on)
            def _():
                kv_send(which, jnp.maximum(z - s, 0), s, True).wait_send()

            @pl.when(jnp.logical_and(dn_on, s < dn_hops))
            def _():
                kv_send(which, (z + s) % zn, s, False).wait_send()

        return carry

    lax.fori_loop(0, up_hops, drain, 0)


def solution(mesh):
    zn = mesh.shape["sp"] // Y

    def per_device(
        normed,
        query_weight,
        key_weight,
        value_weight,
        pool_in_weight,
        pool_weight,
        map_balance,
        head_gain,
        contrast_out_weight,
        pool_out_weight,
    ):
        vmem = pl.BlockSpec(memory_space=pltpu.VMEM)
        hbm = pl.BlockSpec(memory_space=pl.ANY)
        smem = pl.BlockSpec(memory_space=pltpu.SMEM)
        dma = pltpu.SemaphoreType.DMA
        V = pltpu.VMEM
        return pl.pallas_call(
            functools.partial(kernel, zn),
            out_shape=jax.ShapeDtypeStruct(normed.shape, BF16),
            in_specs=[vmem, hbm, hbm, hbm, hbm, vmem, smem, vmem, hbm, hbm],
            out_specs=vmem,
            scratch_shapes=[
                V((8, 2, 16, 2048), BF16),
                V((2048, 256), BF16),
                V((2048, 256), BF16),
                V((2048, 256), BF16),
                V((2048, 128), BF16),
                V((256, 2048), BF16),
                V((128, 2048), BF16),
                V((Y, 2, 128, 256), BF16),
                V((zn, 256, 256), BF16),
                V((zn, 256, 256), BF16),
                V((Y, 2, 256, 256), F32),
                V((Y, 2, 256, 128), F32),
                V((Y, 2, 256, 128), F32),
                V((256, 128), BF16),
                V((16, 128), BF16),
                V((272, 128), F32),
                V((256, 2048), F32),
                V((6, 128, 512), BF16),
                V((6, 8, 128), F32),
                V((2, 128, 512), BF16),
                V((2, 8, 128), F32),
                V((2, 2, 128, 512), BF16),
                V((2, 2, 8, 128), F32),
                V((256, 256), BF16),
                V((X, 2, 2, 16, 2048), BF16),
                V((X, 2, 16, 2048), BF16),
                V((6, 16, 2048), BF16),
                V((2, 16, 2048), BF16),
                V((2, 2, 16, 2048), BF16),
                dma((6,)),
                dma((14,)),
                dma((8, 2)),
                dma((zn // 2, 2)),
                dma((zn // 2, 2)),
                dma((zn, 2)),
                dma((zn, 2)),
                dma((6,)),
                dma((Y, 2)),
                dma((2,)),
                dma((6, 2)),
                dma((6, 2)),
                dma((X,)),
                dma((X,)),
                dma((6,)),
                dma((6,)),
            ],
            compiler_params=pltpu.CompilerParams(
                collective_id=0, has_side_effects=True, vmem_limit_bytes=50 * 1024 * 1024
            ),
        )(
            normed,
            query_weight,
            key_weight,
            value_weight,
            pool_in_weight,
            pool_weight,
            map_balance,
            head_gain.reshape(1, -1),
            contrast_out_weight,
            pool_out_weight,
        )

    return jax.shard_map(
        per_device,
        mesh=mesh,
        in_specs=(
            P(("sp", "tp"), None),
            P(None, "tp"),
            P(None, "tp"),
            P(None, "tp"),
            P(None, "tp"),
            P("tp", None, None),
            P(),
            P(),
            P("tp", None),
            P("tp", None),
        ),
        out_specs=P(("sp", "tp"), None),
        check_vma=False,
    )
```

```python
import functools
import math

import jax
import jax.numpy as jnp
from jax import lax
from jax.experimental import pallas as pl
from jax.experimental.pallas import tpu as pltpu
from jax.sharding import PartitionSpec as P

MESH = pl.DeviceIdType.MESH
F32 = jnp.float32
BF16 = jnp.bfloat16
Y = 4
X = 4
NEG = -1e30
norm_epsilon = 1e-06


def kernel(
    zn,
    normed_h,
    wq_h,
    wk_h,
    wv_h,
    wp_h,
    pool_weight_h,
    balance_h,
    gain_h,
    cow_h,
    pow_h,
    out,
    xg,
    wkv,
    wq,
    wp,
    cow,
    pow_,
    pool_weight,
    gain,
    balance,
    q_all,
    kv_all,
    acc,
    m_s,
    l_s,
    pin,
    rim,
    ext,
    pool_part,
    ps,
    pst,
    r2,
    r2t,
    rn,
    rnt,
    co,
    part,
    pr,
    xs,
    xr2,
    xrn,
    w_sem,
    xg_send,
    xg_recv,
    up_send,
    dn_send,
    kv_up_recv,
    kv_dn_recv,
    q_send,
    q_recv,
    h_sem,
    ps_send,
    ps_recv,
    pr_send,
    pr_recv,
    xs_send,
    xs_recv,
):
    sp = lax.axis_index("sp")
    tp = lax.axis_index("tp")
    nsp = zn * Y
    z, y = sp // Y, sp % Y
    x, core = tp // 2, tp % 2
    hops = zn // 2

    def at(zz, yy, xx, cc):
        return {"sp": zz * Y + yy, "tp": xx * 2 + cc}

    partner = at(z, y, x, 1 - core)
    xr, xl = (x + 1) % X, (x + X - 1) % X
    x2 = (x + 2) % X
    yr, yl = (y + 1) % Y, (y + Y - 1) % Y
    y2 = (y + 2) % Y
    zu, zd = (z + 1) % zn, (z + zn - 1) % zn
    x_right, x_left = at(z, y, xr, core), at(z, y, xl, core)
    y_right, y_left = at(z, yr, x, core), at(z, yl, x, core)
    z_up, z_down = at(zu, y, x, core), at(zd, y, x, core)
    next_sp = {"sp": (sp + 1) % nsp, "tp": tp}
    prev_sp = {"sp": (sp + nsp - 1) % nsp, "tp": tp}

    weights = [
        pltpu.make_async_copy(src, dst, w_sem.at[i])
        for i, (src, dst) in enumerate(
            (
                (wk_h, wkv.at[:, pl.ds(0, 256)]),
                (wv_h, wkv.at[:, pl.ds(256, 256)]),
                (wq_h, wq),
                (wp_h, wp),
                (pow_h, pow_),
                (cow_h, cow),
                (pool_weight_h, pool_weight),
                (gain_h, gain),
                (balance_h, balance),
            )
        )
    ]
    rows_in = [
        pltpu.make_async_copy(
            normed_h.at[pl.ds(16 * half, 16)], xg.at[tp, half], w_sem.at[len(weights) + half]
        )
        for half in range(2)
    ]
    for copy in rows_in + weights:
        copy.start()
    barrier = pltpu.get_barrier_semaphore()
    peers = (partner, x_right, x_left, y_right, y_left, z_up, z_down, next_sp, prev_sp)
    for peer in peers:
        pl.semaphore_signal(barrier, inc=1, device_id=peer, device_id_type=MESH)
    pl.semaphore_wait(barrier, len(peers))
    for copy in rows_in:
        copy.wait()

    def remote(src, dst, send, recv, device):
        return pltpu.make_async_remote_copy(
            src_ref=src,
            dst_ref=dst,
            send_sem=send,
            recv_sem=recv,
            device_id=device,
            device_id_type=MESH,
        )
    sent = []

    def send_x(src, slot, half, device):
        copy = remote(src, xg.at[slot, half], xg_send.at[len(sent)], xg_recv.at[slot, half], device)
        copy.start()
        sent.append(copy)

    def got_x(slot, half):
        remote(
            xg.at[slot, half],
            xg.at[slot, half],
            xg_send.at[0],
            xg_recv.at[slot, half],
            partner,
        ).wait_recv()

    def own(half):
        return xg.at[tp, half]

    send_x(own(0), tp, 0, x_right)
    send_x(own(1), tp, 1, x_left)
    send_x(own(0), tp, 0, partner)
    send_x(own(1), tp, 1, partner)
    send_x(own(1), tp, 1, x_right)
    send_x(own(0), tp, 0, x_left)

    order = (x, xl, xr, x2)

    def kv_copy(slot, i, hop, up):
        piece = kv_all.at[slot, order[i]]
        return remote(
            piece,
            piece,
            (up_send if up else dn_send).at[hop, i],
            (kv_up_recv if up else kv_dn_recv).at[slot, i],
            z_up if up else z_down,
        )

    def sends(s, i):
        up = jnp.logical_and(s <= z, z < zn - 1)
        up = jnp.logical_and(up, s + 1 <= (hops if i < 2 else hops - 1))
        dn = (z + s) % zn <= (hops - 1 if i >= 2 else hops - 2)
        dn = jnp.logical_and(dn, s + 1 <= (hops if i >= 2 else hops - 1))
        return up, dn

    def kv_start(s, i):
        up, dn = sends(s, i)

        @pl.when(up)
        def _():
            kv_copy(jnp.maximum(z - s, 0), i, s, True).start()

        @pl.when(dn)
        def _():
            kv_copy((z + s) % zn, i, s, False).start()

    def pass_on(s, i):
        up_here = jnp.logical_and(s <= z, s <= (hops if i < 2 else hops - 1))
        dn_here = (z + s) % zn <= (hops - 1 if i >= 2 else hops - 2)
        dn_here = jnp.logical_and(dn_here, s <= (hops if i >= 2 else hops - 1))
        up, dn = sends(s, i)

        @pl.when(up_here)
        def _():
            kv_copy(jnp.maximum(z - s, 0), i, 0, True).wait_recv()

        @pl.when(up)
        def _():
            kv_copy(jnp.maximum(z - s, 0), i, s, True).start()

        @pl.when(dn_here)
        def _():
            kv_copy((z + s) % zn, i, 0, False).wait_recv()

        @pl.when(dn)
        def _():
            kv_copy((z + s) % zn, i, s, False).start()

    def project(rows, weight):
        return jnp.dot(rows, weight[...], preferred_element_type=F32).astype(BF16)

    def project_kv(i):
        chip = order[i]
        rows = xg[pl.ds(2 * chip, 2)].reshape(64, 2048)
        kv_all[z, chip] = project(rows, wkv)
        kv_start(0, i)

    from_left, from_right, from_far = 2 * xl + core, 2 * xr + core, 2 * x2 + core

    def got_chip(chip):
        for half in range(2):
            got_x(2 * chip + 1 - core, half)
    for j in range(Y):
        for c in range(2):
            m_s[j, c] = jnp.full((256, 128), NEG, F32)
            l_s[j, c] = jnp.zeros((256, 128), F32)
            acc[j, c] = jnp.zeros((256, 256), F32)
    weights[0].wait()
    weights[1].wait()
    got_chip(x)
    project_kv(0)
    got_x(from_left, 0)
    send_x(xg.at[from_left, 0], from_left, 0, x_right)
    got_x(from_right, 1)
    send_x(xg.at[from_right, 1], from_right, 1, x_left)
    send_x(xg.at[from_left, 0], from_left, 0, partner)
    send_x(xg.at[from_right, 1], from_right, 1, partner)
    got_x(from_left, 1)
    send_x(xg.at[from_left, 1], from_left, 1, partner)
    got_x(from_right, 0)
    send_x(xg.at[from_right, 0], from_right, 0, partner)
    got_chip(xl)
    project_kv(1)
    got_x(from_far, 0)
    send_x(xg.at[from_far, 0], from_far, 0, partner)
    got_x(from_far, 1)
    send_x(xg.at[from_far, 1], from_far, 1, partner)
    got_chip(xr)
    project_kv(2)
    got_chip(x2)
    project_kv(3)

    q_sent = []

    def send_q(slot, half, device):
        copy = remote(
            q_all.at[slot, half],
            q_all.at[slot, half],
            q_send.at[len(q_sent)],
            q_recv.at[slot, half],
            device,
        )
        copy.start()
        q_sent.append(copy)

    def got_q(slot, half):
        remote(
            q_all.at[slot, half],
            q_all.at[slot, half],
            q_send.at[0],
            q_recv.at[slot, half],
            y_right,
        ).wait_recv()
    weights[2].wait()
    whole_rows = xg[...].reshape(256, 2048)
    q_all[y] = project(whole_rows, wq).reshape(2, 128, 256)
    send_q(y, 0, y_right)
    send_q(y, 1, y_left)
    send_q(y, 1, y_right)
    send_q(y, 0, y_left)
    weights[3].wait()
    pin[...] = project(whole_rows, wp)
    halo = remote(pin.at[pl.ds(240, 16)], rim, h_sem.at[0], h_sem.at[1], next_sp)
    halo.start()
    factor = 128 ** (-0.5) * math.log2(math.e)

    def attend(j, slot, masked):
        for c in range(2):
            cols = slice(128 * c, 128 * c + 128)
            q = q_all[j].reshape(256, 256)[:, cols]
            k = kv_all[slot].reshape(256, 512)[:, cols]
            v = kv_all[slot].reshape(256, 512)[:, 256:]
            s = lax.dot_general(q, k, (((1,), (1,)), ((), ())), preferred_element_type=F32) * factor
            if masked:
                row = lax.broadcasted_iota(jnp.int32, (256, 256), 0)
                col = lax.broadcasted_iota(jnp.int32, (256, 256), 1)
                s = jnp.where(col <= row, s, NEG)
            before = m_s[j, c]
            peak = jnp.maximum(before, jnp.max(s, axis=1, keepdims=True))
            shrink = jnp.exp2(before - peak)
            p = jnp.exp2(s - jnp.concatenate([peak, peak], axis=1))
            m_s[j, c] = peak
            l_s[j, c] = l_s[j, c] * shrink + jnp.sum(p, axis=1, keepdims=True)
            pv = jnp.dot(p.astype(BF16), v, preferred_element_type=F32)
            acc[j, c] = acc[j, c] * jnp.concatenate([shrink, shrink], axis=1) + pv

    def work(u):
        first = u < Y
        s = (u - Y) // 8 + 1
        k = jnp.where(first, u, (u - Y) % 8)
        up = k < Y
        near = k % Y
        j = (y + jnp.where(near == 3, 0, jnp.where(near == 2, 3, 2 - near))) % Y
        slot = jnp.where(first, z, jnp.where(up, jnp.maximum(z - s, 0), (z + s) % zn))
        below = jnp.logical_and(up, s <= z)
        above = jnp.logical_and(z + s >= zn, jnp.logical_and(s < hops, jnp.logical_not(up)))
        wanted = jnp.where(first, j > y, jnp.logical_or(below, above))

        @pl.when(wanted)
        def _():
            attend(j, slot, False)

    def work_until(done, ready, most):
        count = jnp.minimum(ready - done, most)

        def one(i, carry):
            work(done + i)
            return carry

        lax.fori_loop(0, count, one, 0)
        return done + count

    pass_on(1, 0)
    pass_on(1, 1)
    attend(y, z, True)
    pass_on(1, 2)
    halo.wait()
    ext[pl.ds(0, 16), :] = jnp.where(sp > 0, rim[...].astype(F32), 0.0)
    ext[pl.ds(16, 256), :] = pin[...].astype(F32)
    width = jnp.left_shift(jnp.int32(2), tp % 4)
    window = jnp.zeros((256, 128), F32)
    for offset in range(16):
        window = window + jnp.where(offset < width, ext[pl.ds(16 - offset, 256), :], 0.0)
    position = sp * 256 + lax.broadcasted_iota(jnp.int32, (256, 128), 0)
    counts = jnp.minimum(position + 1, width).astype(F32)
    spread = (window / counts - ext[pl.ds(16, 256), :]).astype(BF16)
    weights[6].wait()
    pool_out = jnp.dot(spread, pool_weight[0], preferred_element_type=F32).astype(BF16)
    weights[4].wait()
    for n in range(8):
        cols = slice(256 * n, 256 * n + 256)
        pool_part[:, cols] = jnp.dot(pool_out, pow_[:, cols], preferred_element_type=F32)
    for copy in weights[5:]:
        if copy is not weights[6]:
            copy.wait()
    pass_on(1, 3)
    got_q(yl, 0)
    send_q(yl, 0, y_right)
    got_q(yr, 1)
    send_q(yr, 1, y_left)
    pass_on(2, 0)
    got_q(yl, 1)
    got_q(yr, 0)
    pass_on(2, 1)
    got_q(y2, 0)
    got_q(y2, 1)
    done = work_until(0, 4 + 8, 3)
    pass_on(2, 2)
    done = work_until(done, 4 + 8, 3)
    pass_on(2, 3)
    done = work_until(done, 4 + 16, 3)

    def ring_step(s, done):
        for i in range(4):
            pass_on(s, i)
            done = work_until(done, Y + 8 * (s if i == 3 else s - 1), 3)
        return done

    done = lax.fori_loop(3, hops, ring_step, done)
    pass_on(hops, 0)
    pass_on(hops, 2)
    done = work_until(done, Y + 8 * (hops - 1), 3)
    pass_on(hops, 1)
    pass_on(hops, 3)
    work_until(done, Y + 8 * (hops - 1), 99)
    def state(j, half):
        rows = pl.ds(128 * half, 128)
        return [(m_s[j, c, rows, :], l_s[j, c, rows, :], acc[j, c, rows, :]) for c in range(2)]

    def arrived(payload, stats):
        columns = jnp.concatenate([stats[...], jnp.zeros((120, 128), F32)], axis=0).T
        return [
            (
                jnp.broadcast_to(columns[:, 2 * c : 2 * c + 1], (128, 128)),
                jnp.broadcast_to(columns[:, 2 * c + 1 : 2 * c + 2], (128, 128)),
                payload[:, 256 * c : 256 * c + 256].astype(F32),
            )
            for c in range(2)
        ]

    def joined(first, second):
        result = []
        for (m1, l1, a1), (m2, l2, a2) in zip(first, second):
            peak = jnp.maximum(m1, m2)
            s1, s2 = jnp.exp2(m1 - peak), jnp.exp2(m2 - peak)
            wide1 = jnp.concatenate([s1, s1], axis=1)
            wide2 = jnp.concatenate([s2, s2], axis=1)
            result.append((peak, l1 * s1 + l2 * s2, a1 * wide1 + a2 * wide2))
        return result

    y_sent = []

    def send_state(values, index, payload, stats, device):
        (m0, l0, a0), (m1, l1, a1) = values
        lane = lax.broadcasted_iota(jnp.int32, (128, 128), 1)
        table = jnp.where(lane == 0, m0, jnp.where(lane == 1, l0, jnp.where(lane == 2, m1, l1)))
        pst[index] = table.T[:8]
        ps[index, :, :256] = a0.astype(BF16)
        ps[index, :, 256:] = a1.astype(BF16)
        for i, (src, dst) in enumerate(((ps, payload), (pst, stats))):
            copy = remote(src.at[index], dst, ps_send.at[index, i], ps_recv.at[index, i], device)
            copy.start()
            y_sent.append(copy)

    def got_state(index, payload, stats):
        for i, (src, dst) in enumerate(((ps, payload), (pst, stats))):
            remote(
                src.at[index], dst, ps_send.at[index, i], ps_recv.at[index, i], y_right
            ).wait_recv()

    base = Y + 8 * (hops - 1)
    work(base)
    send_state(state(y2, 0), 0, r2.at[0], r2t.at[0], y_right)
    send_state(state(y2, 1), 1, r2.at[1], r2t.at[1], y_left)
    work(base + 1)
    send_state(state(yr, 1), 2, rn.at[0, 1], rnt.at[0, 1], y_right)
    work(base + 2)
    send_state(state(yl, 0), 3, rn.at[1, 0], rnt.at[1, 0], y_left)
    work(base + 3)
    got_state(0, r2.at[0], r2t.at[0])
    send_state(
        joined(state(yr, 0), arrived(r2.at[0], r2t.at[0])), 4, rn.at[0, 0], rnt.at[0, 0], y_right
    )
    got_state(1, r2.at[1], r2t.at[1])
    send_state(
        joined(state(yl, 1), arrived(r2.at[1], r2t.at[1])), 5, rn.at[1, 1], rnt.at[1, 1], y_left
    )
    level = balance[tp]
    got_state(2, rn.at[0, 1], rnt.at[0, 1])
    got_state(3, rn.at[1, 0], rnt.at[1, 0])
    for half in range(2):
        if half == 0:
            got_state(4, rn.at[0, 0], rnt.at[0, 0])
        else:
            got_state(5, rn.at[1, 1], rnt.at[1, 1])
        whole = state(y, half)
        for side in range(2):
            whole = joined(whole, arrived(rn.at[side, half], rnt.at[side, half]))
        maps = [
            (a / jnp.concatenate([l, l], axis=1)).astype(BF16).astype(F32) for _, l, a in whole
        ]
        contrast = maps[0] - level * maps[1]
        square = jnp.mean(contrast * contrast, axis=1, keepdims=True)
        contrast = contrast * lax.rsqrt(square + norm_epsilon) * gain[...]
        co[pl.ds(128 * half, 128), :] = contrast.astype(BF16)
    mixed = co[...]
    for n in range(8):
        cols = slice(256 * n, 256 * n + 256)
        tile = jnp.dot(mixed, cow[:, cols], preferred_element_type=F32) + pool_part[:, cols]
        part[:, :, :, :, cols] = tile.astype(BF16).reshape(X, 2, 2, 16, 256)
    pair = [
        remote(part.at[xx, 1 - core], pr.at[xx], pr_send.at[xx], pr_recv.at[xx], partner)
        for xx in range(X)
    ]
    for copy in pair:
        copy.start()
    for copy in pair:
        copy.wait_recv()
    def both(owner, half):
        return part[owner, core, half].astype(F32) + pr[owner, half].astype(F32)

    x_sent = []

    def send_sum(value, index, dst, device):
        xs[index] = value.astype(BF16)
        copy = remote(xs.at[index], dst, xs_send.at[index], xs_recv.at[index], device)
        copy.start()
        x_sent.append(copy)

    def got_sum(index, dst):
        remote(xs.at[index], dst, xs_send.at[index], xs_recv.at[index], x_right).wait_recv()

    send_sum(both(x2, 0), 0, xr2.at[0], x_right)
    send_sum(both(x2, 1), 1, xr2.at[1], x_left)
    send_sum(both(xr, 1), 2, xrn.at[0, 1], x_right)
    send_sum(both(xl, 0), 3, xrn.at[1, 0], x_left)
    got_sum(0, xr2.at[0])
    send_sum(both(xr, 0) + xr2[0].astype(F32), 4, xrn.at[0, 0], x_right)
    got_sum(1, xr2.at[1])
    send_sum(both(xl, 1) + xr2[1].astype(F32), 5, xrn.at[1, 1], x_left)
    got_sum(2, xrn.at[0, 1])
    got_sum(3, xrn.at[1, 0])
    got_sum(4, xrn.at[0, 0])
    got_sum(5, xrn.at[1, 1])
    for half in range(2):
        total = both(x, half) + xrn[0, half].astype(F32) + xrn[1, half].astype(F32)
        out[pl.ds(16 * half, 16), :] = total.astype(BF16)
    for copy in sent + q_sent + y_sent + pair + x_sent:
        copy.wait_send()

    def drain(s, carry):
        for i in range(4):
            up, dn = sends(s, i)

            @pl.when(up)
            def _():
                kv_copy(jnp.maximum(z - s, 0), i, s, True).wait_send()

            @pl.when(dn)
            def _():
                kv_copy((z + s) % zn, i, s, False).wait_send()

        return carry

    lax.fori_loop(0, hops, drain, 0)


def solution(mesh):
    zn = mesh.shape["sp"] // Y

    def per_device(
        normed,
        query_weight,
        key_weight,
        value_weight,
        pool_in_weight,
        pool_weight,
        map_balance,
        head_gain,
        contrast_out_weight,
        pool_out_weight,
    ):
        vmem = pl.BlockSpec(memory_space=pltpu.VMEM)
        hbm = pl.BlockSpec(memory_space=pl.ANY)
        dma = pltpu.SemaphoreType.DMA
        V = pltpu.VMEM
        return pl.pallas_call(
            functools.partial(kernel, zn),
            out_shape=jax.ShapeDtypeStruct(normed.shape, BF16),
            in_specs=[hbm] * 10,
            out_specs=vmem,
            scratch_shapes=[
                V((8, 2, 16, 2048), BF16),
                V((2048, 512), BF16),
                V((2048, 256), BF16),
                V((2048, 128), BF16),
                V((256, 2048), BF16),
                V((128, 2048), BF16),
                V((1, 128, 128), BF16),
                V((1, 256), F32),
                pltpu.SMEM((8,), F32),
                V((Y, 2, 128, 256), BF16),
                V((zn, X, 64, 512), BF16),
                V((Y, 2, 256, 256), F32),
                V((Y, 2, 256, 128), F32),
                V((Y, 2, 256, 128), F32),
                V((256, 128), BF16),
                V((16, 128), BF16),
                V((272, 128), F32),
                V((256, 2048), F32),
                V((6, 128, 512), BF16),
                V((6, 8, 128), F32),
                V((2, 128, 512), BF16),
                V((2, 8, 128), F32),
                V((2, 2, 128, 512), BF16),
                V((2, 2, 8, 128), F32),
                V((256, 256), BF16),
                V((X, 2, 2, 16, 2048), BF16),
                V((X, 2, 16, 2048), BF16),
                V((6, 16, 2048), BF16),
                V((2, 16, 2048), BF16),
                V((2, 2, 16, 2048), BF16),
                dma((11,)),
                dma((14,)),
                dma((8, 2)),
                dma((zn // 2, X)),
                dma((zn // 2, X)),
                dma((zn, X)),
                dma((zn, X)),
                dma((6,)),
                dma((Y, 2)),
                dma((2,)),
                dma((6, 2)),
                dma((6, 2)),
                dma((X,)),
                dma((X,)),
                dma((6,)),
                dma((6,)),
            ],
            compiler_params=pltpu.CompilerParams(
                collective_id=0, has_side_effects=True, vmem_limit_bytes=67043328
            ),
        )(
            normed,
            query_weight,
            key_weight,
            value_weight,
            pool_in_weight,
            pool_weight,
            map_balance,
            head_gain.reshape(1, -1),
            contrast_out_weight,
            pool_out_weight,
        )

    return jax.shard_map(
        per_device,
        mesh=mesh,
        in_specs=(
            P(("sp", "tp"), None),
            P(None, "tp"),
            P(None, "tp"),
            P(None, "tp"),
            P(None, "tp"),
            P("tp", None, None),
            P(),
            P(),
            P("tp", None),
            P("tp", None),
        ),
        out_specs=P(("sp", "tp"), None),
        check_vma=False,
    )
```

```python
import functools
import math

import jax
import jax.numpy as jnp
from jax import lax
from jax.experimental import pallas as pl
from jax.experimental.pallas import tpu as pltpu
from jax.sharding import PartitionSpec as P

MESH = pl.DeviceIdType.MESH
F32 = jnp.float32
BF16 = jnp.bfloat16
Y = 4
X = 4
NEG = -1e30
norm_epsilon = 1e-06


def kernel(
    zn,
    normed_h,
    wq_h,
    wk_h,
    wv_h,
    wp_h,
    pool_weight_h,
    balance_h,
    gain_h,
    cow_h,
    pow_h,
    out,
    xg,
    wkv,
    wq,
    wp,
    cow,
    pow_,
    pool_weight,
    gain,
    balance,
    q_all,
    kv_all,
    acc,
    m_s,
    l_s,
    pin,
    rim,
    ext,
    pool_part,
    ps,
    pst,
    r2,
    r2t,
    rn,
    rnt,
    co,
    part,
    pr,
    xs,
    xr2,
    xrn,
    w_sem,
    xg_send,
    xg_recv,
    up_send,
    dn_send,
    kv_recv,
    q_send,
    q_recv,
    h_sem,
    ps_send,
    ps_recv,
    pr_send,
    pr_recv,
    xs_send,
    xs_recv,
):
    sp = lax.axis_index("sp")
    tp = lax.axis_index("tp")
    nsp = zn * Y
    z, y = sp // Y, sp % Y
    x, core = tp // 2, tp % 2
    hops = zn // 2

    def at(zz, yy, xx, cc):
        return {"sp": zz * Y + yy, "tp": xx * 2 + cc}

    partner = at(z, y, x, 1 - core)
    xr, xl = (x + 1) % X, (x + X - 1) % X
    x2 = (x + 2) % X
    yr, yl = (y + 1) % Y, (y + Y - 1) % Y
    y2 = (y + 2) % Y
    zu, zd = (z + 1) % zn, (z + zn - 1) % zn
    x_right, x_left = at(z, y, xr, core), at(z, y, xl, core)
    y_right, y_left = at(z, yr, x, core), at(z, yl, x, core)
    z_up, z_down = at(zu, y, x, core), at(zd, y, x, core)
    next_sp = {"sp": (sp + 1) % nsp, "tp": tp}
    prev_sp = {"sp": (sp + nsp - 1) % nsp, "tp": tp}

    weights = [
        pltpu.make_async_copy(src, dst, w_sem.at[i])
        for i, (src, dst) in enumerate(
            (
                (wk_h, wkv.at[:, pl.ds(0, 256)]),
                (wv_h, wkv.at[:, pl.ds(256, 256)]),
                (wq_h, wq),
                (wp_h, wp),
                (pow_h, pow_),
                (cow_h, cow),
                (pool_weight_h, pool_weight),
                (gain_h, gain),
                (balance_h, balance),
            )
        )
    ]
    rows_in = [
        pltpu.make_async_copy(
            normed_h.at[pl.ds(16 * half, 16)], xg.at[tp, half], w_sem.at[len(weights) + half]
        )
        for half in range(2)
    ]
    for copy in rows_in + weights:
        copy.start()
    barrier = pltpu.get_barrier_semaphore()
    peers = (partner, x_right, x_left, y_right, y_left, z_up, z_down, next_sp, prev_sp)
    for peer in peers:
        pl.semaphore_signal(barrier, inc=1, device_id=peer, device_id_type=MESH)
    pl.semaphore_wait(barrier, len(peers))
    for copy in rows_in:
        copy.wait()

    def remote(src, dst, send, recv, device):
        return pltpu.make_async_remote_copy(
            src_ref=src,
            dst_ref=dst,
            send_sem=send,
            recv_sem=recv,
            device_id=device,
            device_id_type=MESH,
        )
    sent = []

    def send_x(src, slot, half, device):
        copy = remote(src, xg.at[slot, half], xg_send.at[len(sent)], xg_recv.at[slot, half], device)
        copy.start()
        sent.append(copy)

    def got_x(slot, half):
        remote(
            xg.at[slot, half],
            xg.at[slot, half],
            xg_send.at[0],
            xg_recv.at[slot, half],
            partner,
        ).wait_recv()

    def own(half):
        return xg.at[tp, half]

    send_x(own(0), tp, 0, x_right)
    send_x(own(1), tp, 1, x_left)
    send_x(own(0), tp, 0, partner)
    send_x(own(1), tp, 1, partner)
    send_x(own(1), tp, 1, x_right)
    send_x(own(0), tp, 0, x_left)

    order = (x, xl, xr, x2)

    def kv_copy(slot, i, hop, up):
        piece = kv_all.at[slot, order[i]]
        return remote(
            piece,
            piece,
            (up_send if up else dn_send).at[hop % 2, i],
            kv_recv.at[slot, i],
            z_up if up else z_down,
        )

    def sends(s, i):
        up = jnp.logical_and(s <= z, z < zn - 1)
        up = jnp.logical_and(up, s + 1 <= (hops if i < 2 else hops - 1))
        dn = (z + s) % zn <= (hops - 1 if i >= 2 else hops - 2)
        dn = jnp.logical_and(dn, s + 1 <= (hops if i >= 2 else hops - 1))
        return up, dn

    def kv_left(s, i):
        up, dn = sends(s, i)

        @pl.when(up)
        def _():
            kv_copy(jnp.maximum(z - s, 0), i, s, True).wait_send()

        @pl.when(dn)
        def _():
            kv_copy((z + s) % zn, i, s, False).wait_send()

    def kv_start(s, i):
        up, dn = sends(s, i)

        @pl.when(up)
        def _():
            kv_copy(jnp.maximum(z - s, 0), i, s, True).start()

        @pl.when(dn)
        def _():
            kv_copy((z + s) % zn, i, s, False).start()

    def pass_on(s, i):
        up_here = jnp.logical_and(s <= z, s <= (hops if i < 2 else hops - 1))
        dn_here = (z + s) % zn <= (hops - 1 if i >= 2 else hops - 2)
        dn_here = jnp.logical_and(dn_here, s <= (hops if i >= 2 else hops - 1))
        up, dn = sends(s, i)
        if not (isinstance(s, int) and s < 2):
            kv_left(s - 2, i)

        @pl.when(up_here)
        def _():
            kv_copy(jnp.maximum(z - s, 0), i, 0, True).wait_recv()

        @pl.when(up)
        def _():
            kv_copy(jnp.maximum(z - s, 0), i, s, True).start()

        @pl.when(dn_here)
        def _():
            kv_copy((z + s) % zn, i, 0, False).wait_recv()

        @pl.when(dn)
        def _():
            kv_copy((z + s) % zn, i, s, False).start()

    def project(rows, weight):
        return jnp.dot(rows, weight[...], preferred_element_type=F32).astype(BF16)

    def project_kv(i):
        chip = order[i]
        rows = xg[pl.ds(2 * chip, 2)].reshape(64, 2048)
        kv_all[z, chip] = project(rows, wkv)
        kv_start(0, i)

    q_sent = []

    def q_copy(slot, i, device, send):
        piece = q_all.at[slot, order[i]]
        return remote(piece, piece, q_send.at[send], q_recv.at[slot, i], device)

    def send_q(slot, i, device):
        copy = q_copy(slot, i, device, len(q_sent))
        copy.start()
        q_sent.append(copy)

    def got_q(slot, i):
        q_copy(slot, i, y_right, 0).wait_recv()

    def project_q(i):
        chip = order[i]
        rows = xg[pl.ds(2 * chip, 2)].reshape(64, 2048)
        q_all[y, chip] = project(rows, wq)
        send_q(y, i, y_right)
        send_q(y, i, y_left)

    def relay_q(i):
        if i % 2 == 0:
            got_q(yl, i)
            send_q(yl, i, y_right)
        else:
            got_q(yr, i)
            send_q(yr, i, y_left)

    from_left, from_right, from_far = 2 * xl + core, 2 * xr + core, 2 * x2 + core

    def got_chip(chip):
        for half in range(2):
            got_x(2 * chip + 1 - core, half)
    for j in range(Y):
        for c in range(2):
            m_s[j, c] = jnp.full((256, 128), NEG, F32)
            l_s[j, c] = jnp.zeros((256, 128), F32)
            acc[j, c] = jnp.zeros((256, 256), F32)
    weights[0].wait()
    weights[1].wait()
    got_chip(x)
    project_kv(0)
    weights[2].wait()
    project_q(0)
    got_x(from_left, 0)
    send_x(xg.at[from_left, 0], from_left, 0, x_right)
    got_x(from_right, 1)
    send_x(xg.at[from_right, 1], from_right, 1, x_left)
    send_x(xg.at[from_left, 0], from_left, 0, partner)
    send_x(xg.at[from_right, 1], from_right, 1, partner)
    got_x(from_left, 1)
    send_x(xg.at[from_left, 1], from_left, 1, partner)
    got_x(from_right, 0)
    send_x(xg.at[from_right, 0], from_right, 0, partner)
    pass_on(1, 0)
    got_chip(xl)
    project_kv(1)
    got_x(from_far, 0)
    send_x(xg.at[from_far, 0], from_far, 0, partner)
    got_x(from_far, 1)
    send_x(xg.at[from_far, 1], from_far, 1, partner)
    project_q(1)
    got_chip(xr)
    project_kv(2)
    got_chip(x2)
    project_kv(3)
    project_q(2)
    project_q(3)
    pass_on(1, 1)

    whole_rows = xg[...].reshape(256, 2048)
    weights[3].wait()
    pin[...] = project(whole_rows, wp)
    halo = remote(pin.at[pl.ds(240, 16)], rim, h_sem.at[0], h_sem.at[1], next_sp)
    halo.start()
    factor = 128 ** (-0.5) * math.log2(math.e)

    def attend(j, slot, masked):
        for c in range(2):
            cols = slice(128 * c, 128 * c + 128)
            q = q_all[j].reshape(256, 256)[:, cols]
            k = kv_all[slot].reshape(256, 512)[:, cols]
            v = kv_all[slot].reshape(256, 512)[:, 256:]
            s = lax.dot_general(q, k, (((1,), (1,)), ((), ())), preferred_element_type=F32) * factor
            if masked:
                row = lax.broadcasted_iota(jnp.int32, (256, 256), 0)
                col = lax.broadcasted_iota(jnp.int32, (256, 256), 1)
                s = jnp.where(col <= row, s, NEG)
            before = m_s[j, c]
            peak = jnp.maximum(before, jnp.max(s, axis=1, keepdims=True))
            shrink = jnp.exp2(before - peak)
            p = jnp.exp2(s - jnp.concatenate([peak, peak], axis=1))
            m_s[j, c] = peak
            l_s[j, c] = l_s[j, c] * shrink + (p[:, :128] + p[:, 128:])
            pv = jnp.dot(p.astype(BF16), v, preferred_element_type=F32)
            acc[j, c] = acc[j, c] * jnp.concatenate([shrink, shrink], axis=1) + pv

    partners = (y2, yr, yl, y)

    def work(u, group):
        s = u // 2 + 1
        up = u % 2 == 0
        slot = jnp.where(up, jnp.maximum(z - s, 0), (z + s) % zn)
        below = jnp.logical_and(up, s <= z)
        above = jnp.logical_and(z + s >= zn, jnp.logical_and(s < hops, jnp.logical_not(up)))

        @pl.when(jnp.logical_or(below, above))
        def _():
            for j in group:
                attend(j, slot, False)

    def work_once(done, ready):
        @pl.when(done < ready)
        def _():
            work(done, partners)

        return jnp.minimum(done + 1, ready)

    def pooling():
        halo.wait()
        ext[pl.ds(0, 16), :] = jnp.where(sp > 0, rim[...].astype(F32), 0.0)
        ext[pl.ds(16, 256), :] = pin[...].astype(F32)
        width = jnp.left_shift(jnp.int32(2), tp % 4)
        window = jnp.zeros((256, 128), F32)
        for offset in range(16):
            window = window + jnp.where(offset < width, ext[pl.ds(16 - offset, 256), :], 0.0)
        position = sp * 256 + lax.broadcasted_iota(jnp.int32, (256, 128), 0)
        counts = jnp.minimum(position + 1, width).astype(F32)
        spread = (window / counts - ext[pl.ds(16, 256), :]).astype(BF16)
        weights[6].wait()
        pool_out = jnp.dot(spread, pool_weight[0], preferred_element_type=F32).astype(BF16)
        weights[4].wait()
        for n in range(8):
            cols = slice(256 * n, 256 * n + 256)
            pool_part[:, cols] = jnp.dot(pool_out, pow_[:, cols], preferred_element_type=F32)
        for copy in weights[5:]:
            if copy is not weights[6]:
                copy.wait()
    pass_on(2, 0)
    relay_q(0)
    relay_q(1)
    attend(y, z, True)
    pass_on(1, 2)
    relay_q(2)
    relay_q(3)
    pass_on(1, 3)
    for i in range(4):
        if i % 2 == 0:
            got_q(yr, i)
        else:
            got_q(yl, i)
    for i in range(4):
        got_q(y2, i)
    def own_step(j, carry):
        @pl.when(j > y)
        def _():
            attend(j, z, False)

        return carry

    lax.fori_loop(0, Y, own_step, 0)

    def ring_step(s, done):
        pass_on(s, 1)
        done = work_once(done, 2 * (s - 1))
        pass_on(s + 1, 0)
        done = work_once(done, 2 * (s - 1))
        pass_on(s, 2)
        done = work_once(done, 2 * (s - 1))

        @pl.when(s == hops // 2 + 1)
        def _():
            pooling()
        pass_on(s, 3)
        return done

    done = lax.fori_loop(2, hops, ring_step, 0)
    pass_on(hops, 2)
    done = work_once(done, 2 * (hops - 1))
    pass_on(hops, 1)
    done = lax.fori_loop(
        done, 2 * (hops - 1), lambda i, d: work_once(d, 2 * (hops - 1)), done
    )
    pass_on(hops, 3)
    def state(j, half):
        rows = pl.ds(128 * half, 128)
        return [
            (
                m_s[j, c, rows, :],
                jnp.broadcast_to(jnp.sum(l_s[j, c, rows, :], axis=1, keepdims=True), (128, 128)),
                acc[j, c, rows, :],
            )
            for c in range(2)
        ]

    def arrived(payload, stats):
        columns = jnp.concatenate([stats[...], jnp.zeros((120, 128), F32)], axis=0).T
        return [
            (
                jnp.broadcast_to(columns[:, 2 * c : 2 * c + 1], (128, 128)),
                jnp.broadcast_to(columns[:, 2 * c + 1 : 2 * c + 2], (128, 128)),
                payload[:, 256 * c : 256 * c + 256].astype(F32),
            )
            for c in range(2)
        ]

    def joined(first, second):
        result = []
        for (m1, l1, a1), (m2, l2, a2) in zip(first, second):
            peak = jnp.maximum(m1, m2)
            s1, s2 = jnp.exp2(m1 - peak), jnp.exp2(m2 - peak)
            wide1 = jnp.concatenate([s1, s1], axis=1)
            wide2 = jnp.concatenate([s2, s2], axis=1)
            result.append((peak, l1 * s1 + l2 * s2, a1 * wide1 + a2 * wide2))
        return result

    y_sent = []

    def send_state(values, index, payload, stats, device):
        (m0, l0, a0), (m1, l1, a1) = values
        lane = lax.broadcasted_iota(jnp.int32, (128, 128), 1)
        table = jnp.where(lane == 0, m0, jnp.where(lane == 1, l0, jnp.where(lane == 2, m1, l1)))
        pst[index] = table.T[:8]
        ps[index, :, :256] = a0.astype(BF16)
        ps[index, :, 256:] = a1.astype(BF16)
        for i, (src, dst) in enumerate(((ps, payload), (pst, stats))):
            copy = remote(src.at[index], dst, ps_send.at[index, i], ps_recv.at[index, i], device)
            copy.start()
            y_sent.append(copy)

    def got_state(index, payload, stats):
        for i, (src, dst) in enumerate(((ps, payload), (pst, stats))):
            remote(
                src.at[index], dst, ps_send.at[index, i], ps_recv.at[index, i], y_right
            ).wait_recv()

    base = 2 * (hops - 1)
    work(base, (y2, yr))
    send_state(state(y2, 0), 0, r2.at[0], r2t.at[0], y_right)
    send_state(state(y2, 1), 1, r2.at[1], r2t.at[1], y_left)
    send_state(state(yr, 1), 2, rn.at[0, 1], rnt.at[0, 1], y_right)
    work(base, (yl, y))
    send_state(state(yl, 0), 3, rn.at[1, 0], rnt.at[1, 0], y_left)
    got_state(0, r2.at[0], r2t.at[0])
    send_state(
        joined(state(yr, 0), arrived(r2.at[0], r2t.at[0])), 4, rn.at[0, 0], rnt.at[0, 0], y_right
    )
    got_state(1, r2.at[1], r2t.at[1])
    send_state(
        joined(state(yl, 1), arrived(r2.at[1], r2t.at[1])), 5, rn.at[1, 1], rnt.at[1, 1], y_left
    )
    level = balance[tp]
    got_state(2, rn.at[0, 1], rnt.at[0, 1])
    got_state(3, rn.at[1, 0], rnt.at[1, 0])
    for half in range(2):
        if half == 0:
            got_state(4, rn.at[0, 0], rnt.at[0, 0])
        else:
            got_state(5, rn.at[1, 1], rnt.at[1, 1])
        whole = state(y, half)
        for side in range(2):
            whole = joined(whole, arrived(rn.at[side, half], rnt.at[side, half]))
        maps = [
            (a / jnp.concatenate([l, l], axis=1)).astype(BF16).astype(F32) for _, l, a in whole
        ]
        contrast = maps[0] - level * maps[1]
        square = jnp.mean(contrast * contrast, axis=1, keepdims=True)
        contrast = contrast * lax.rsqrt(square + norm_epsilon) * gain[...]
        co[pl.ds(128 * half, 128), :] = contrast.astype(BF16)
    mixed = co[...]
    for n in range(8):
        cols = slice(256 * n, 256 * n + 256)
        tile = jnp.dot(mixed, cow[:, cols], preferred_element_type=F32) + pool_part[:, cols]
        part[:, :, :, :, cols] = tile.astype(BF16).reshape(X, 2, 2, 16, 256)
    pair = remote(part.at[:, 1 - core], pr, pr_send.at[0], pr_recv.at[0], partner)
    pair.start()
    pair.wait_recv()
    def both(owner, half):
        return part[owner, core, half].astype(F32) + pr[owner, half].astype(F32)

    x_sent = []

    def send_sum(value, index, dst, device):
        xs[index] = value.astype(BF16)
        copy = remote(xs.at[index], dst, xs_send.at[index], xs_recv.at[index], device)
        copy.start()
        x_sent.append(copy)

    def got_sum(index, dst):
        remote(xs.at[index], dst, xs_send.at[index], xs_recv.at[index], x_right).wait_recv()

    send_sum(both(x2, 0), 0, xr2.at[0], x_right)
    send_sum(both(x2, 1), 1, xr2.at[1], x_left)
    send_sum(both(xr, 1), 2, xrn.at[0, 1], x_right)
    send_sum(both(xl, 0), 3, xrn.at[1, 0], x_left)
    got_sum(0, xr2.at[0])
    send_sum(both(xr, 0) + xr2[0].astype(F32), 4, xrn.at[0, 0], x_right)
    got_sum(1, xr2.at[1])
    send_sum(both(xl, 1) + xr2[1].astype(F32), 5, xrn.at[1, 1], x_left)
    got_sum(2, xrn.at[0, 1])
    got_sum(3, xrn.at[1, 0])
    got_sum(4, xrn.at[0, 0])
    got_sum(5, xrn.at[1, 1])
    for half in range(2):
        total = both(x, half) + xrn[0, half].astype(F32) + xrn[1, half].astype(F32)
        out[pl.ds(16 * half, 16), :] = total.astype(BF16)
    for copy in sent + q_sent + y_sent + [pair] + x_sent:
        copy.wait_send()

    for i in range(4):
        kv_left(hops - 1, i)


def solution(mesh):
    zn = mesh.shape["sp"] // Y

    def per_device(
        normed,
        query_weight,
        key_weight,
        value_weight,
        pool_in_weight,
        pool_weight,
        map_balance,
        head_gain,
        contrast_out_weight,
        pool_out_weight,
    ):
        vmem = pl.BlockSpec(memory_space=pltpu.VMEM)
        hbm = pl.BlockSpec(memory_space=pl.ANY)
        dma = pltpu.SemaphoreType.DMA
        V = pltpu.VMEM
        return pl.pallas_call(
            functools.partial(kernel, zn),
            out_shape=jax.ShapeDtypeStruct(normed.shape, BF16),
            in_specs=[hbm] * 10,
            out_specs=vmem,
            scratch_shapes=[
                V((8, 2, 16, 2048), BF16),
                V((2048, 512), BF16),
                V((2048, 256), BF16),
                V((2048, 128), BF16),
                V((256, 2048), BF16),
                V((128, 2048), BF16),
                V((1, 128, 128), BF16),
                V((1, 256), F32),
                pltpu.SMEM((8,), F32),
                V((Y, X, 64, 256), BF16),
                V((zn, X, 64, 512), BF16),
                V((Y, 2, 256, 256), F32),
                V((Y, 2, 256, 128), F32),
                V((Y, 2, 256, 128), F32),
                V((256, 128), BF16),
                V((16, 128), BF16),
                V((272, 128), F32),
                V((256, 2048), F32),
                V((6, 128, 512), BF16),
                V((6, 8, 128), F32),
                V((2, 128, 512), BF16),
                V((2, 8, 128), F32),
                V((2, 2, 128, 512), BF16),
                V((2, 2, 8, 128), F32),
                V((256, 256), BF16),
                V((X, 2, 2, 16, 2048), BF16),
                V((X, 2, 16, 2048), BF16),
                V((6, 16, 2048), BF16),
                V((2, 16, 2048), BF16),
                V((2, 2, 16, 2048), BF16),
                dma((11,)),
                dma((14,)),
                dma((8, 2)),
                dma((2, X)),
                dma((2, X)),
                dma((zn, X)),
                dma((12,)),
                dma((Y, X)),
                dma((2,)),
                dma((6, 2)),
                dma((6, 2)),
                dma((1,)),
                dma((1,)),
                dma((6,)),
                dma((6,)),
            ],
            compiler_params=pltpu.CompilerParams(
                collective_id=0, has_side_effects=True, vmem_limit_bytes=67043328
            ),
        )(
            normed,
            query_weight,
            key_weight,
            value_weight,
            pool_in_weight,
            pool_weight,
            map_balance,
            head_gain.reshape(1, -1),
            contrast_out_weight,
            pool_out_weight,
        )

    return jax.shard_map(
        per_device,
        mesh=mesh,
        in_specs=(
            P(("sp", "tp"), None),
            P(None, "tp"),
            P(None, "tp"),
            P(None, "tp"),
            P(None, "tp"),
            P("tp", None, None),
            P(),
            P(),
            P("tp", None),
            P("tp", None),
        ),
        out_specs=P(("sp", "tp"), None),
        check_vma=False,
    )
```

```python
import functools
import math

import jax
import jax.numpy as jnp
from jax import lax
from jax.experimental import pallas as pl
from jax.experimental.pallas import tpu as pltpu
from jax.sharding import PartitionSpec as P

MESH = pl.DeviceIdType.MESH
F32 = jnp.float32
BF16 = jnp.bfloat16
Y = 4
X = 4
NEG = -1e30
norm_epsilon = 1e-06


def kernel(
    zn,
    normed_h,
    wq_h,
    wk_h,
    wv_h,
    wp_h,
    pool_weight_h,
    balance_h,
    gain_h,
    cow_h,
    pow_h,
    out,
    xg,
    wkv,
    wq,
    wp,
    cow,
    pow_,
    pool_weight,
    gain,
    balance,
    q_all,
    kv_all,
    acc,
    m_s,
    l_s,
    pin,
    rim,
    ext,
    pool_part,
    ps,
    pst,
    r2,
    r2t,
    rn,
    rnt,
    co,
    part,
    pr,
    xs,
    xr2,
    xrn,
    w_sem,
    xg_send,
    xg_recv,
    up_send,
    dn_send,
    kv_recv,
    q_send,
    q_recv,
    h_sem,
    ps_send,
    ps_recv,
    pr_send,
    pr_recv,
    xs_send,
    xs_recv,
):
    sp = lax.axis_index("sp")
    tp = lax.axis_index("tp")
    nsp = zn * Y
    z, y = sp // Y, sp % Y
    x, core = tp // 2, tp % 2
    hops = zn // 2

    def at(zz, yy, xx, cc):
        return {"sp": zz * Y + yy, "tp": xx * 2 + cc}

    partner = at(z, y, x, 1 - core)
    xr, xl = (x + 1) % X, (x + X - 1) % X
    x2 = (x + 2) % X
    yr, yl = (y + 1) % Y, (y + Y - 1) % Y
    y2 = (y + 2) % Y
    zu, zd = (z + 1) % zn, (z + zn - 1) % zn
    x_right, x_left = at(z, y, xr, core), at(z, y, xl, core)
    y_right, y_left = at(z, yr, x, core), at(z, yl, x, core)
    z_up, z_down = at(zu, y, x, core), at(zd, y, x, core)
    next_sp = {"sp": (sp + 1) % nsp, "tp": tp}
    prev_sp = {"sp": (sp + nsp - 1) % nsp, "tp": tp}

    weights = [
        pltpu.make_async_copy(src, dst, w_sem.at[i])
        for i, (src, dst) in enumerate(
            (
                (wk_h, wkv.at[:, pl.ds(0, 256)]),
                (wv_h, wkv.at[:, pl.ds(256, 256)]),
                (wq_h, wq),
                (wp_h, wp),
                (pow_h, pow_),
                (cow_h, cow),
                (pool_weight_h, pool_weight),
                (gain_h, gain),
                (balance_h, balance),
            )
        )
    ]
    rows_in = [
        pltpu.make_async_copy(
            normed_h.at[pl.ds(16 * half, 16)], xg.at[tp, half], w_sem.at[len(weights) + half]
        )
        for half in range(2)
    ]
    for copy in rows_in + weights:
        copy.start()
    barrier = pltpu.get_barrier_semaphore()
    peers = (partner, x_right, x_left, y_right, y_left, z_up, z_down, next_sp, prev_sp)
    for peer in peers:
        pl.semaphore_signal(barrier, inc=1, device_id=peer, device_id_type=MESH)
    pl.semaphore_wait(barrier, len(peers))
    for copy in rows_in:
        copy.wait()

    def remote(src, dst, send, recv, device):
        return pltpu.make_async_remote_copy(
            src_ref=src,
            dst_ref=dst,
            send_sem=send,
            recv_sem=recv,
            device_id=device,
            device_id_type=MESH,
        )
    sent = []

    def send_x(src, slot, half, device):
        copy = remote(src, xg.at[slot, half], xg_send.at[len(sent)], xg_recv.at[slot, half], device)
        copy.start()
        sent.append(copy)

    def got_x(slot, half):
        remote(
            xg.at[slot, half],
            xg.at[slot, half],
            xg_send.at[0],
            xg_recv.at[slot, half],
            partner,
        ).wait_recv()

    def own(half):
        return xg.at[tp, half]

    send_x(own(0), tp, 0, x_right)
    send_x(own(1), tp, 1, x_left)
    send_x(own(0), tp, 0, partner)
    send_x(own(1), tp, 1, partner)
    send_x(own(1), tp, 1, x_right)
    send_x(own(0), tp, 0, x_left)

    order = (x, xl, xr, x2)

    def kv_copy(slot, i, hop, up):
        piece = kv_all.at[slot, order[i]]
        return remote(
            piece,
            piece,
            (up_send if up else dn_send).at[hop % 2, i],
            kv_recv.at[slot, i],
            z_up if up else z_down,
        )

    def sends(s, i):
        up = jnp.logical_and(s <= z, z < zn - 1)
        up = jnp.logical_and(up, s + 1 <= (hops if i < 2 else hops - 1))
        dn = (z + s) % zn <= (hops - 1 if i >= 2 else hops - 2)
        dn = jnp.logical_and(dn, s + 1 <= (hops if i >= 2 else hops - 1))
        return up, dn

    def kv_left(s, i):
        up, dn = sends(s, i)

        @pl.when(up)
        def _():
            kv_copy(jnp.maximum(z - s, 0), i, s, True).wait_send()

        @pl.when(dn)
        def _():
            kv_copy((z + s) % zn, i, s, False).wait_send()

    def kv_start(s, i):
        up, dn = sends(s, i)

        @pl.when(up)
        def _():
            kv_copy(jnp.maximum(z - s, 0), i, s, True).start()

        @pl.when(dn)
        def _():
            kv_copy((z + s) % zn, i, s, False).start()

    def pass_on(s, i):
        up_here = jnp.logical_and(s <= z, s <= (hops if i < 2 else hops - 1))
        dn_here = (z + s) % zn <= (hops - 1 if i >= 2 else hops - 2)
        dn_here = jnp.logical_and(dn_here, s <= (hops if i >= 2 else hops - 1))
        up, dn = sends(s, i)
        if not (isinstance(s, int) and s < 2):
            kv_left(s - 2, i)

        @pl.when(up_here)
        def _():
            kv_copy(jnp.maximum(z - s, 0), i, 0, True).wait_recv()

        @pl.when(up)
        def _():
            kv_copy(jnp.maximum(z - s, 0), i, s, True).start()

        @pl.when(dn_here)
        def _():
            kv_copy((z + s) % zn, i, 0, False).wait_recv()

        @pl.when(dn)
        def _():
            kv_copy((z + s) % zn, i, s, False).start()

    def project(rows, weight):
        return jnp.dot(rows, weight[...], preferred_element_type=F32).astype(BF16)

    def project_kv(i):
        chip = order[i]
        rows = xg[pl.ds(2 * chip, 2)].reshape(64, 2048)
        kv_all[z, chip] = project(rows, wkv)
        kv_start(0, i)

    q_sent = []

    def q_copy(slot, i, device, send):
        piece = q_all.at[slot, order[i]]
        return remote(piece, piece, q_send.at[send], q_recv.at[slot, i], device)

    def send_q(slot, i, device):
        copy = q_copy(slot, i, device, len(q_sent))
        copy.start()
        q_sent.append(copy)

    def got_q(slot, i):
        q_copy(slot, i, y_right, 0).wait_recv()

    def project_q(i):
        chip = order[i]
        rows = xg[pl.ds(2 * chip, 2)].reshape(64, 2048)
        q_all[y, chip] = project(rows, wq)
        send_q(y, i, y_right)
        send_q(y, i, y_left)

    def relay_q(i):
        if i % 2 == 0:
            got_q(yl, i)
            send_q(yl, i, y_right)
        else:
            got_q(yr, i)
            send_q(yr, i, y_left)

    from_left, from_right, from_far = 2 * xl + core, 2 * xr + core, 2 * x2 + core

    def got_chip(chip):
        for half in range(2):
            got_x(2 * chip + 1 - core, half)
    for j in range(Y):
        for c in range(2):
            m_s[j, c] = jnp.full((256, 128), NEG, F32)
            l_s[j, c] = jnp.zeros((256, 128), F32)
            acc[j, c] = jnp.zeros((256, 256), F32)
    weights[0].wait()
    weights[1].wait()
    got_chip(x)
    project_kv(0)
    weights[2].wait()
    project_q(0)
    got_x(from_left, 0)
    send_x(xg.at[from_left, 0], from_left, 0, x_right)
    got_x(from_right, 1)
    send_x(xg.at[from_right, 1], from_right, 1, x_left)
    send_x(xg.at[from_left, 0], from_left, 0, partner)
    send_x(xg.at[from_right, 1], from_right, 1, partner)
    pass_on(1, 0)
    got_x(from_left, 1)
    send_x(xg.at[from_left, 1], from_left, 1, partner)
    got_x(from_right, 0)
    send_x(xg.at[from_right, 0], from_right, 0, partner)
    got_chip(xl)
    project_kv(1)
    got_x(from_far, 0)
    send_x(xg.at[from_far, 0], from_far, 0, partner)
    got_x(from_far, 1)
    send_x(xg.at[from_far, 1], from_far, 1, partner)
    project_q(1)
    got_chip(xr)
    project_kv(2)
    pass_on(2, 0)
    got_chip(x2)
    project_kv(3)
    project_q(2)
    project_q(3)
    pass_on(1, 1)

    whole_rows = xg[...].reshape(256, 2048)
    weights[3].wait()
    pin[...] = project(whole_rows, wp)
    halo = remote(pin.at[pl.ds(240, 16)], rim, h_sem.at[0], h_sem.at[1], next_sp)
    halo.start()
    factor = 128 ** (-0.5) * math.log2(math.e)

    def attend(j, slot, masked):
        for c in range(2):
            cols = slice(128 * c, 128 * c + 128)
            q = q_all[j].reshape(256, 256)[:, cols]
            k = kv_all[slot].reshape(256, 512)[:, cols]
            v = kv_all[slot].reshape(256, 512)[:, 256:]
            s = lax.dot_general(q, k, (((1,), (1,)), ((), ())), preferred_element_type=F32) * factor
            if masked:
                row = lax.broadcasted_iota(jnp.int32, (256, 256), 0)
                col = lax.broadcasted_iota(jnp.int32, (256, 256), 1)
                s = jnp.where(col <= row, s, NEG)
            before = m_s[j, c]
            peak = jnp.maximum(before, jnp.max(s, axis=1, keepdims=True))
            shrink = jnp.exp2(before - peak)
            p = jnp.exp2(s - jnp.concatenate([peak, peak], axis=1))
            m_s[j, c] = peak
            l_s[j, c] = l_s[j, c] * shrink + (p[:, :128] + p[:, 128:])
            pv = jnp.dot(p.astype(BF16), v, preferred_element_type=F32)
            acc[j, c] = acc[j, c] * jnp.concatenate([shrink, shrink], axis=1) + pv

    partners = (y2, yr, yl, y)

    def work(u, group):
        s = u // 2 + 1
        up = u % 2 == 0
        slot = jnp.where(up, jnp.maximum(z - s, 0), (z + s) % zn)
        below = jnp.logical_and(up, s <= z)
        above = jnp.logical_and(z + s >= zn, jnp.logical_and(s < hops, jnp.logical_not(up)))

        @pl.when(jnp.logical_or(below, above))
        def _():
            for j in group:
                attend(j, slot, False)

    def work_once(done, ready):
        @pl.when(done < ready)
        def _():
            work(done, partners)

        return jnp.minimum(done + 1, ready)

    def pooling():
        halo.wait()
        ext[pl.ds(0, 16), :] = jnp.where(sp > 0, rim[...].astype(F32), 0.0)
        ext[pl.ds(16, 256), :] = pin[...].astype(F32)
        width = jnp.left_shift(jnp.int32(2), tp % 4)
        window = jnp.zeros((256, 128), F32)
        for offset in range(16):
            window = window + jnp.where(offset < width, ext[pl.ds(16 - offset, 256), :], 0.0)
        position = sp * 256 + lax.broadcasted_iota(jnp.int32, (256, 128), 0)
        counts = jnp.minimum(position + 1, width).astype(F32)
        spread = (window / counts - ext[pl.ds(16, 256), :]).astype(BF16)
        weights[6].wait()
        pool_out = jnp.dot(spread, pool_weight[0], preferred_element_type=F32).astype(BF16)
        weights[4].wait()
        for n in range(8):
            cols = slice(256 * n, 256 * n + 256)
            pool_part[:, cols] = jnp.dot(pool_out, pow_[:, cols], preferred_element_type=F32)
        for copy in weights[5:]:
            if copy is not weights[6]:
                copy.wait()
    relay_q(0)
    relay_q(1)
    attend(y, z, True)
    pass_on(1, 2)
    relay_q(2)
    relay_q(3)
    pass_on(3, 0)
    pass_on(1, 3)
    for i in range(4):
        if i % 2 == 0:
            got_q(yr, i)
        else:
            got_q(yl, i)
    for i in range(4):
        got_q(y2, i)
    def own_step(j, carry):
        @pl.when(j > y)
        def _():
            attend(j, z, False)

        return carry

    lax.fori_loop(0, Y, own_step, 0)

    def ring_step(s, done):
        pass_on(s, 1)
        done = work_once(done, 2 * (s - 1))
        pass_on(s + 2, 0)
        done = work_once(done, 2 * (s - 1))
        pass_on(s, 2)
        done = work_once(done, 2 * (s - 1))

        @pl.when(s == hops // 2 + 1)
        def _():
            pooling()
        pass_on(s, 3)
        return done

    done = lax.fori_loop(2, hops, ring_step, 0)
    done = work_once(done, 2 * (hops - 1))
    pass_on(hops, 2)
    done = work_once(done, 2 * (hops - 1))
    pass_on(hops, 1)
    done = lax.fori_loop(
        done, 2 * (hops - 1), lambda i, d: work_once(d, 2 * (hops - 1)), done
    )
    pass_on(hops, 3)
    def state(j, half):
        rows = pl.ds(128 * half, 128)
        return [
            (
                m_s[j, c, rows, :],
                jnp.broadcast_to(jnp.sum(l_s[j, c, rows, :], axis=1, keepdims=True), (128, 128)),
                acc[j, c, rows, :],
            )
            for c in range(2)
        ]

    def arrived(payload, stats):
        columns = jnp.concatenate([stats[...], jnp.zeros((120, 128), F32)], axis=0).T
        return [
            (
                jnp.broadcast_to(columns[:, 2 * c : 2 * c + 1], (128, 128)),
                jnp.broadcast_to(columns[:, 2 * c + 1 : 2 * c + 2], (128, 128)),
                payload[:, 256 * c : 256 * c + 256].astype(F32),
            )
            for c in range(2)
        ]

    def joined(first, second):
        result = []
        for (m1, l1, a1), (m2, l2, a2) in zip(first, second):
            peak = jnp.maximum(m1, m2)
            s1, s2 = jnp.exp2(m1 - peak), jnp.exp2(m2 - peak)
            wide1 = jnp.concatenate([s1, s1], axis=1)
            wide2 = jnp.concatenate([s2, s2], axis=1)
            result.append((peak, l1 * s1 + l2 * s2, a1 * wide1 + a2 * wide2))
        return result

    y_sent = []

    def send_state(values, index, payload, stats, device):
        (m0, l0, a0), (m1, l1, a1) = values
        lane = lax.broadcasted_iota(jnp.int32, (128, 128), 1)
        table = jnp.where(lane == 0, m0, jnp.where(lane == 1, l0, jnp.where(lane == 2, m1, l1)))
        pst[index] = table.T[:8]
        ps[index, :, :256] = a0.astype(BF16)
        ps[index, :, 256:] = a1.astype(BF16)
        for i, (src, dst) in enumerate(((ps, payload), (pst, stats))):
            copy = remote(src.at[index], dst, ps_send.at[index, i], ps_recv.at[index, i], device)
            copy.start()
            y_sent.append(copy)

    def got_state(index, payload, stats):
        for i, (src, dst) in enumerate(((ps, payload), (pst, stats))):
            remote(
                src.at[index], dst, ps_send.at[index, i], ps_recv.at[index, i], y_right
            ).wait_recv()

    base = 2 * (hops - 1)
    work(base, (y2, yr))
    send_state(state(y2, 0), 0, r2.at[0], r2t.at[0], y_right)
    send_state(state(y2, 1), 1, r2.at[1], r2t.at[1], y_left)
    send_state(state(yr, 1), 2, rn.at[0, 1], rnt.at[0, 1], y_right)
    work(base, (yl, y))
    send_state(state(yl, 0), 3, rn.at[1, 0], rnt.at[1, 0], y_left)
    got_state(0, r2.at[0], r2t.at[0])
    send_state(
        joined(state(yr, 0), arrived(r2.at[0], r2t.at[0])), 4, rn.at[0, 0], rnt.at[0, 0], y_right
    )
    got_state(1, r2.at[1], r2t.at[1])
    send_state(
        joined(state(yl, 1), arrived(r2.at[1], r2t.at[1])), 5, rn.at[1, 1], rnt.at[1, 1], y_left
    )
    level = balance[tp]
    got_state(2, rn.at[0, 1], rnt.at[0, 1])
    got_state(3, rn.at[1, 0], rnt.at[1, 0])
    for half in range(2):
        if half == 0:
            got_state(4, rn.at[0, 0], rnt.at[0, 0])
        else:
            got_state(5, rn.at[1, 1], rnt.at[1, 1])
        whole = state(y, half)
        for side in range(2):
            whole = joined(whole, arrived(rn.at[side, half], rnt.at[side, half]))
        maps = [
            (a / jnp.concatenate([l, l], axis=1)).astype(BF16).astype(F32) for _, l, a in whole
        ]
        contrast = maps[0] - level * maps[1]
        square = jnp.mean(contrast * contrast, axis=1, keepdims=True)
        contrast = contrast * lax.rsqrt(square + norm_epsilon) * gain[...]
        co[pl.ds(128 * half, 128), :] = contrast.astype(BF16)
    mixed = co[...]
    for n in range(8):
        cols = slice(256 * n, 256 * n + 256)
        tile = jnp.dot(mixed, cow[:, cols], preferred_element_type=F32) + pool_part[:, cols]
        part[:, :, :, :, cols] = tile.astype(BF16).reshape(X, 2, 2, 16, 256)
    pair = remote(part.at[:, 1 - core], pr, pr_send.at[0], pr_recv.at[0], partner)
    pair.start()
    pair.wait_recv()
    def both(owner, half):
        return part[owner, core, half].astype(F32) + pr[owner, half].astype(F32)

    x_sent = []

    def send_sum(value, index, dst, device):
        xs[index] = value.astype(BF16)
        copy = remote(xs.at[index], dst, xs_send.at[index], xs_recv.at[index], device)
        copy.start()
        x_sent.append(copy)

    def got_sum(index, dst):
        remote(xs.at[index], dst, xs_send.at[index], xs_recv.at[index], x_right).wait_recv()

    send_sum(both(x2, 0), 0, xr2.at[0], x_right)
    send_sum(both(x2, 1), 1, xr2.at[1], x_left)
    send_sum(both(xr, 1), 2, xrn.at[0, 1], x_right)
    send_sum(both(xl, 0), 3, xrn.at[1, 0], x_left)
    got_sum(0, xr2.at[0])
    send_sum(both(xr, 0) + xr2[0].astype(F32), 4, xrn.at[0, 0], x_right)
    got_sum(1, xr2.at[1])
    send_sum(both(xl, 1) + xr2[1].astype(F32), 5, xrn.at[1, 1], x_left)
    got_sum(2, xrn.at[0, 1])
    got_sum(3, xrn.at[1, 0])
    got_sum(4, xrn.at[0, 0])
    got_sum(5, xrn.at[1, 1])
    for half in range(2):
        total = both(x, half) + xrn[0, half].astype(F32) + xrn[1, half].astype(F32)
        out[pl.ds(16 * half, 16), :] = total.astype(BF16)
    for copy in sent + q_sent + y_sent + [pair] + x_sent:
        copy.wait_send()

    for i in range(1, 4):
        kv_left(hops - 1, i)


def solution(mesh):
    zn = mesh.shape["sp"] // Y

    def per_device(
        normed,
        query_weight,
        key_weight,
        value_weight,
        pool_in_weight,
        pool_weight,
        map_balance,
        head_gain,
        contrast_out_weight,
        pool_out_weight,
    ):
        vmem = pl.BlockSpec(memory_space=pltpu.VMEM)
        hbm = pl.BlockSpec(memory_space=pl.ANY)
        dma = pltpu.SemaphoreType.DMA
        V = pltpu.VMEM
        return pl.pallas_call(
            functools.partial(kernel, zn),
            out_shape=pltpu.VMEM(normed.shape, BF16),
            in_specs=[hbm] * 10,
            out_specs=vmem,
            scratch_shapes=[
                V((8, 2, 16, 2048), BF16),
                V((2048, 512), BF16),
                V((2048, 256), BF16),
                V((2048, 128), BF16),
                V((256, 2048), BF16),
                V((128, 2048), BF16),
                V((1, 128, 128), BF16),
                V((1, 256), F32),
                pltpu.SMEM((8,), F32),
                V((Y, X, 64, 256), BF16),
                V((zn, X, 64, 512), BF16),
                V((Y, 2, 256, 256), F32),
                V((Y, 2, 256, 128), F32),
                V((Y, 2, 256, 128), F32),
                V((256, 128), BF16),
                V((16, 128), BF16),
                V((272, 128), F32),
                V((256, 2048), F32),
                V((6, 128, 512), BF16),
                V((6, 8, 128), F32),
                V((2, 128, 512), BF16),
                V((2, 8, 128), F32),
                V((2, 2, 128, 512), BF16),
                V((2, 2, 8, 128), F32),
                V((256, 256), BF16),
                V((X, 2, 2, 16, 2048), BF16),
                V((X, 2, 16, 2048), BF16),
                V((6, 16, 2048), BF16),
                V((2, 16, 2048), BF16),
                V((2, 2, 16, 2048), BF16),
                dma((11,)),
                dma((14,)),
                dma((8, 2)),
                dma((2, X)),
                dma((2, X)),
                dma((zn, X)),
                dma((12,)),
                dma((Y, X)),
                dma((2,)),
                dma((6, 2)),
                dma((6, 2)),
                dma((1,)),
                dma((1,)),
                dma((6,)),
                dma((6,)),
            ],
            compiler_params=pltpu.CompilerParams(
                collective_id=0, has_side_effects=True, vmem_limit_bytes=66900000
            ),
        )(
            normed,
            query_weight,
            key_weight,
            value_weight,
            pool_in_weight,
            pool_weight,
            map_balance,
            head_gain.reshape(1, -1),
            contrast_out_weight,
            pool_out_weight,
        )

    return jax.shard_map(
        per_device,
        mesh=mesh,
        in_specs=(
            P(("sp", "tp"), None),
            P(None, "tp"),
            P(None, "tp"),
            P(None, "tp"),
            P(None, "tp"),
            P("tp", None, None),
            P(),
            P(),
            P("tp", None),
            P("tp", None),
        ),
        out_specs=P(("sp", "tp"), None),
        check_vma=False,
    )
```

```python
import functools
import math

import jax
import jax.numpy as jnp
from jax import lax
from jax.experimental import pallas as pl
from jax.experimental.pallas import tpu as pltpu
from jax.sharding import PartitionSpec as P

MESH = pl.DeviceIdType.MESH
F32 = jnp.float32
BF16 = jnp.bfloat16
Y = 4
X = 4
NEG = -1e30
norm_epsilon = 1e-06


def kernel(
    zn,
    normed_h,
    wq_h,
    wk_h,
    wv_h,
    wp_h,
    pool_weight_h,
    balance_h,
    gain_h,
    cow_h,
    pow_h,
    out,
    xg,
    wkv,
    wq,
    wp,
    cow,
    pow_,
    pool_weight,
    gain,
    balance,
    q_all,
    kv_all,
    acc,
    m_s,
    l_s,
    pin,
    rim,
    ext,
    pool_part,
    ps,
    pst,
    r2,
    r2t,
    rn,
    rnt,
    co,
    part,
    pr,
    xs,
    xr2,
    xrn,
    w_sem,
    xg_send,
    xg_recv,
    up_send,
    dn_send,
    kv_recv,
    q_send,
    q_recv,
    h_sem,
    ps_recv,
    pr_recv,
    xs_recv,
):
    sp = lax.axis_index("sp")
    tp = lax.axis_index("tp")
    nsp = zn * Y
    z, y = sp // Y, sp % Y
    x, core = tp // 2, tp % 2
    hops = zn // 2

    def at(zz, yy, xx, cc):
        return {"sp": zz * Y + yy, "tp": xx * 2 + cc}

    partner = at(z, y, x, 1 - core)
    xr, xl = (x + 1) % X, (x + X - 1) % X
    x2 = (x + 2) % X
    yr, yl = (y + 1) % Y, (y + Y - 1) % Y
    y2 = (y + 2) % Y
    zu, zd = (z + 1) % zn, (z + zn - 1) % zn
    x_right, x_left = at(z, y, xr, core), at(z, y, xl, core)
    y_right, y_left = at(z, yr, x, core), at(z, yl, x, core)
    z_up, z_down = at(zu, y, x, core), at(zd, y, x, core)
    next_sp = {"sp": (sp + 1) % nsp, "tp": tp}
    prev_sp = {"sp": (sp + nsp - 1) % nsp, "tp": tp}

    weights = [
        pltpu.make_async_copy(src, dst, w_sem.at[i])
        for i, (src, dst) in enumerate(
            (
                (wk_h, wkv.at[:, pl.ds(0, 256)]),
                (wv_h, wkv.at[:, pl.ds(256, 256)]),
                (wq_h, wq),
                (wp_h, wp),
                (pow_h, pow_),
                (cow_h, cow),
                (pool_weight_h, pool_weight),
                (gain_h, gain),
                (balance_h, balance),
            )
        )
    ]
    rows_in = [
        pltpu.make_async_copy(
            normed_h.at[pl.ds(16 * half, 16)], xg.at[tp, half], w_sem.at[len(weights) + half]
        )
        for half in range(2)
    ]
    for copy in rows_in + weights:
        copy.start()
    barrier = pltpu.get_barrier_semaphore()
    peers = (partner, x_right, x_left, y_right, y_left, z_up, z_down, next_sp, prev_sp)
    for peer in peers:
        pl.semaphore_signal(barrier, inc=1, device_id=peer, device_id_type=MESH)
    pl.semaphore_wait(barrier, len(peers))
    for copy in rows_in:
        copy.wait()

    def remote(src, dst, send, recv, device):
        return pltpu.make_async_remote_copy(
            src_ref=src,
            dst_ref=dst,
            send_sem=send,
            recv_sem=recv,
            device_id=device,
            device_id_type=MESH,
        )
    sent = []

    def send_x(src, slot, half, device):
        copy = remote(src, xg.at[slot, half], xg_send.at[len(sent)], xg_recv.at[slot, half], device)
        copy.start()
        sent.append(copy)

    def got_x(slot, half):
        remote(
            xg.at[slot, half],
            xg.at[slot, half],
            xg_send.at[0],
            xg_recv.at[slot, half],
            partner,
        ).wait_recv()

    def own(half):
        return xg.at[tp, half]

    send_x(own(0), tp, 0, x_right)
    send_x(own(1), tp, 1, x_left)
    send_x(own(0), tp, 0, partner)
    send_x(own(1), tp, 1, partner)
    send_x(own(1), tp, 1, x_right)
    send_x(own(0), tp, 0, x_left)

    order = (x, xl, xr, x2)

    def kv_copy(slot, i, hop, up):
        piece = kv_all.at[slot, order[i]]
        return remote(
            piece,
            piece,
            (up_send if up else dn_send).at[hop % 2, i],
            kv_recv.at[slot, i],
            z_up if up else z_down,
        )

    def sends(s, i):
        up = jnp.logical_and(s <= z, z < zn - 1)
        up = jnp.logical_and(up, s + 1 <= (hops if i < 2 else hops - 1))
        dn = (z + s) % zn <= (hops - 1 if i >= 2 else hops - 2)
        dn = jnp.logical_and(dn, s + 1 <= (hops if i >= 2 else hops - 1))
        return up, dn

    def left_up(s, i):
        @pl.when(sends(s, i)[0])
        def _():
            kv_copy(jnp.maximum(z - s, 0), i, s, True).wait_send()

    def left_down(s, i):
        @pl.when(sends(s, i)[1])
        def _():
            kv_copy((z + s) % zn, i, s, False).wait_send()

    def kv_start(s, i):
        up, dn = sends(s, i)

        @pl.when(up)
        def _():
            kv_copy(jnp.maximum(z - s, 0), i, s, True).start()

        @pl.when(dn)
        def _():
            kv_copy((z + s) % zn, i, s, False).start()

    def pass_up(s, i):
        here = jnp.logical_and(s <= z, s <= (hops if i < 2 else hops - 1))
        if not (isinstance(s, int) and s < 2):
            left_up(s - 2, i)

        @pl.when(here)
        def _():
            kv_copy(jnp.maximum(z - s, 0), i, 0, True).wait_recv()

        @pl.when(sends(s, i)[0])
        def _():
            kv_copy(jnp.maximum(z - s, 0), i, s, True).start()

    def pass_down(s, i):
        here = (z + s) % zn <= (hops - 1 if i >= 2 else hops - 2)
        here = jnp.logical_and(here, s <= (hops if i >= 2 else hops - 1))
        if not (isinstance(s, int) and s < 2):
            left_down(s - 2, i)

        @pl.when(here)
        def _():
            kv_copy((z + s) % zn, i, 0, False).wait_recv()

        @pl.when(sends(s, i)[1])
        def _():
            kv_copy((z + s) % zn, i, s, False).start()

    def pass_on(s, i):
        pass_up(s, i)
        pass_down(s, i)

    def project(rows, weight):
        return jnp.dot(rows, weight[...], preferred_element_type=F32).astype(BF16)

    def project_kv(i):
        chip = order[i]
        rows = xg[pl.ds(2 * chip, 2)].reshape(64, 2048)
        kv_all[z, chip] = project(rows, wkv)
        kv_start(0, i)

    q_sent = []

    def q_copy(slot, i, device, send):
        piece = q_all.at[slot, order[i]]
        return remote(piece, piece, q_send.at[send], q_recv.at[slot, i], device)

    def send_q(slot, i, device):
        copy = q_copy(slot, i, device, len(q_sent))
        copy.start()
        q_sent.append(copy)

    def got_q(slot, i):
        q_copy(slot, i, y_right, 0).wait_recv()

    def project_q(i):
        chip = order[i]
        rows = xg[pl.ds(2 * chip, 2)].reshape(64, 2048)
        q_all[y, chip] = project(rows, wq)
        send_q(y, i, y_right)
        send_q(y, i, y_left)

    def relay_q(i):
        if i % 2 == 0:
            got_q(yl, i)
            send_q(yl, i, y_right)
        else:
            got_q(yr, i)
            send_q(yr, i, y_left)

    from_left, from_right, from_far = 2 * xl + core, 2 * xr + core, 2 * x2 + core

    def got_chip(chip):
        for half in range(2):
            got_x(2 * chip + 1 - core, half)
    for j in range(Y):
        for c in range(2):
            m_s[j, c] = jnp.full((256, 128), NEG, F32)
            l_s[j, c] = jnp.zeros((256, 128), F32)
            acc[j, c] = jnp.zeros((256, 256), F32)
    weights[0].wait()
    weights[1].wait()
    got_chip(x)
    project_kv(0)
    weights[2].wait()
    project_q(0)
    got_x(from_left, 0)
    send_x(xg.at[from_left, 0], from_left, 0, x_right)
    got_x(from_right, 1)
    send_x(xg.at[from_right, 1], from_right, 1, x_left)
    send_x(xg.at[from_left, 0], from_left, 0, partner)
    send_x(xg.at[from_right, 1], from_right, 1, partner)
    pass_on(1, 0)
    got_x(from_left, 1)
    send_x(xg.at[from_left, 1], from_left, 1, partner)
    got_x(from_right, 0)
    send_x(xg.at[from_right, 0], from_right, 0, partner)
    got_chip(xl)
    project_kv(1)
    got_x(from_far, 0)
    send_x(xg.at[from_far, 0], from_far, 0, partner)
    got_x(from_far, 1)
    send_x(xg.at[from_far, 1], from_far, 1, partner)
    project_q(1)
    got_chip(xr)
    project_kv(2)
    pass_on(2, 0)
    got_chip(x2)
    project_kv(3)
    project_q(2)
    project_q(3)
    pass_on(1, 1)

    whole_rows = xg[...].reshape(256, 2048)
    weights[3].wait()
    pin[...] = project(whole_rows, wp)
    halo = remote(pin.at[pl.ds(240, 16)], rim, h_sem.at[0], h_sem.at[1], next_sp)
    halo.start()
    factor = 128 ** (-0.5) * math.log2(math.e)

    def attend(j, slot, masked):
        for c in range(2):
            cols = slice(128 * c, 128 * c + 128)
            q = q_all[j].reshape(256, 256)[:, cols]
            k = kv_all[slot].reshape(256, 512)[:, cols]
            v = kv_all[slot].reshape(256, 512)[:, 256:]
            s = lax.dot_general(q, k, (((1,), (1,)), ((), ())), preferred_element_type=F32) * factor
            if masked:
                row = lax.broadcasted_iota(jnp.int32, (256, 256), 0)
                col = lax.broadcasted_iota(jnp.int32, (256, 256), 1)
                s = jnp.where(col <= row, s, NEG)
            before = m_s[j, c]
            peak = jnp.maximum(before, jnp.max(s, axis=1, keepdims=True))
            shrink = jnp.exp2(before - peak)
            p = jnp.exp2(s - jnp.concatenate([peak, peak], axis=1))
            m_s[j, c] = peak
            l_s[j, c] = l_s[j, c] * shrink + (p[:, :128] + p[:, 128:])
            pv = jnp.dot(p.astype(BF16), v, preferred_element_type=F32)
            acc[j, c] = acc[j, c] * jnp.concatenate([shrink, shrink], axis=1) + pv

    partners = (y2, yr, yl, y)

    def work(u, group):
        s = u // 2 + 1
        up = u % 2 == 0
        slot = jnp.where(up, jnp.maximum(z - s, 0), (z + s) % zn)
        below = jnp.logical_and(up, s <= z)
        above = jnp.logical_and(z + s >= zn, jnp.logical_and(s < hops, jnp.logical_not(up)))

        @pl.when(jnp.logical_or(below, above))
        def _():
            for j in group:
                attend(j, slot, False)

    def work_once(done, ready):
        @pl.when(done < ready)
        def _():
            work(done, partners)

        return jnp.minimum(done + 1, ready)

    def pooling():
        halo.wait()
        ext[pl.ds(0, 16), :] = jnp.where(sp > 0, rim[...].astype(F32), 0.0)
        ext[pl.ds(16, 256), :] = pin[...].astype(F32)
        width = jnp.left_shift(jnp.int32(2), tp % 4)
        window = jnp.zeros((256, 128), F32)
        for offset in range(16):
            window = window + jnp.where(offset < width, ext[pl.ds(16 - offset, 256), :], 0.0)
        position = sp * 256 + lax.broadcasted_iota(jnp.int32, (256, 128), 0)
        counts = jnp.minimum(position + 1, width).astype(F32)
        spread = (window / counts - ext[pl.ds(16, 256), :]).astype(BF16)
        weights[6].wait()
        pool_out = jnp.dot(spread, pool_weight[0], preferred_element_type=F32).astype(BF16)
        weights[4].wait()
        for n in range(8):
            cols = slice(256 * n, 256 * n + 256)
            pool_part[:, cols] = jnp.dot(pool_out, pow_[:, cols], preferred_element_type=F32)
        for copy in weights[5:]:
            if copy is not weights[6]:
                copy.wait()
    relay_q(0)
    relay_q(1)
    attend(y, z, True)
    pass_on(1, 2)
    relay_q(2)
    relay_q(3)
    pass_on(3, 0)
    pass_on(1, 3)
    for i in range(4):
        if i % 2 == 0:
            got_q(yr, i)
        else:
            got_q(yl, i)
    for i in range(4):
        got_q(y2, i)
    pass_down(2, 1)

    def own_step(j, carry):
        @pl.when(j > y)
        def _():
            attend(j, z, False)

        return carry

    def ring_step(s, done):
        pass_up(s, 1)
        pass_down(s, 2)
        @pl.when(s == 2)
        def _():
            lax.fori_loop(0, Y, own_step, 0)

        done = work_once(done, jnp.where(s == 2, 0, 2 * (s - 1)))
        pass_on(s + 2, 0)
        done = work_once(done, 2 * (s - 1))
        pass_up(s, 2)
        pass_down(s, 3)
        done = work_once(done, 2 * (s - 1))

        @pl.when(s == hops // 2 + 1)
        def _():
            pooling()
        pass_up(s, 3)
        pass_down(s + 1, 1)
        return done

    done = lax.fori_loop(2, hops, ring_step, 0)
    for copy in sent + q_sent:
        copy.wait_send()
    done = work_once(done, 2 * (hops - 1))
    pass_down(hops, 2)
    done = work_once(done, 2 * (hops - 1))
    for i in (1, 2, 3):
        pass_up(hops, i)
    done = lax.fori_loop(
        done, 2 * (hops - 1), lambda i, d: work_once(d, 2 * (hops - 1)), done
    )
    pass_down(hops, 3)
    def state(j, half):
        rows = pl.ds(128 * half, 128)
        return [
            (
                m_s[j, c, rows, :],
                jnp.broadcast_to(jnp.sum(l_s[j, c, rows, :], axis=1, keepdims=True), (128, 128)),
                acc[j, c, rows, :],
            )
            for c in range(2)
        ]

    def arrived(payload, stats):
        columns = jnp.concatenate([stats[...], jnp.zeros((120, 128), F32)], axis=0).T
        return [
            (
                jnp.broadcast_to(columns[:, 2 * c : 2 * c + 1], (128, 128)),
                jnp.broadcast_to(columns[:, 2 * c + 1 : 2 * c + 2], (128, 128)),
                payload[:, 256 * c : 256 * c + 256].astype(F32),
            )
            for c in range(2)
        ]

    def joined(first, second):
        result = []
        for (m1, l1, a1), (m2, l2, a2) in zip(first, second):
            peak = jnp.maximum(m1, m2)
            s1, s2 = jnp.exp2(m1 - peak), jnp.exp2(m2 - peak)
            wide1 = jnp.concatenate([s1, s1], axis=1)
            wide2 = jnp.concatenate([s2, s2], axis=1)
            result.append((peak, l1 * s1 + l2 * s2, a1 * wide1 + a2 * wide2))
        return result

    y_sent = []

    def send_state(values, index, payload, stats, device):
        (m0, l0, a0), (m1, l1, a1) = values
        lane = lax.broadcasted_iota(jnp.int32, (128, 128), 1)
        table = jnp.where(lane == 0, m0, jnp.where(lane == 1, l0, jnp.where(lane == 2, m1, l1)))
        pst[index] = table.T[:8]
        ps[index, :, :256] = a0.astype(BF16)
        ps[index, :, 256:] = a1.astype(BF16)
        for i, (src, dst) in enumerate(((ps, payload), (pst, stats))):
            copy = remote(src.at[index], dst, q_send.at[2 * index + i], ps_recv.at[index, i], device)
            copy.start()
            y_sent.append(copy)

    def got_state(index, payload, stats):
        for i, (src, dst) in enumerate(((ps, payload), (pst, stats))):
            remote(
                src.at[index], dst, q_send.at[2 * index + i], ps_recv.at[index, i], y_right
            ).wait_recv()

    base = 2 * (hops - 1)
    work(base, (y2,))
    send_state(state(y2, 0), 0, r2.at[0], r2t.at[0], y_right)
    send_state(state(y2, 1), 1, r2.at[1], r2t.at[1], y_left)
    work(base, (yr, yl, y))
    send_state(state(yr, 1), 2, rn.at[0, 1], rnt.at[0, 1], y_right)
    send_state(state(yl, 0), 3, rn.at[1, 0], rnt.at[1, 0], y_left)
    got_state(0, r2.at[0], r2t.at[0])
    send_state(
        joined(state(yr, 0), arrived(r2.at[0], r2t.at[0])), 4, rn.at[0, 0], rnt.at[0, 0], y_right
    )
    got_state(1, r2.at[1], r2t.at[1])
    send_state(
        joined(state(yl, 1), arrived(r2.at[1], r2t.at[1])), 5, rn.at[1, 1], rnt.at[1, 1], y_left
    )
    level = balance[tp]
    got_state(2, rn.at[0, 1], rnt.at[0, 1])
    got_state(3, rn.at[1, 0], rnt.at[1, 0])
    for half in range(2):
        if half == 0:
            got_state(4, rn.at[0, 0], rnt.at[0, 0])
        else:
            got_state(5, rn.at[1, 1], rnt.at[1, 1])
        whole = state(y, half)
        for side in range(2):
            whole = joined(whole, arrived(rn.at[side, half], rnt.at[side, half]))
        maps = [
            (a / jnp.concatenate([l, l], axis=1)).astype(BF16).astype(F32) for _, l, a in whole
        ]
        contrast = maps[0] - level * maps[1]
        square = jnp.mean(contrast * contrast, axis=1, keepdims=True)
        contrast = contrast * lax.rsqrt(square + norm_epsilon) * gain[...]
        co[pl.ds(128 * half, 128), :] = contrast.astype(BF16)
    mixed = co[...]
    for n in range(8):
        cols = slice(256 * n, 256 * n + 256)
        tile = jnp.dot(mixed, cow[:, cols], preferred_element_type=F32) + pool_part[:, cols]
        part[:, :, :, :, cols] = tile.astype(BF16).reshape(X, 2, 2, 16, 256)
    pair = [
        remote(
            part.at[chip, 1 - core], pr.at[chip], xg_send.at[6 + i], pr_recv.at[i], partner
        )
        for i, chip in enumerate((x2, xr, xl, x))
    ]
    for copy in pair:
        copy.start()
    pair[0].wait_recv()
    def both(owner, half):
        return part[owner, core, half].astype(F32) + pr[owner, half].astype(F32)

    x_sent = []

    def send_sum(value, index, dst, device):
        xs[index] = value.astype(BF16)
        copy = remote(xs.at[index], dst, xg_send.at[index], xs_recv.at[index], device)
        copy.start()
        x_sent.append(copy)

    def got_sum(index, dst):
        remote(xs.at[index], dst, xg_send.at[index], xs_recv.at[index], x_right).wait_recv()

    send_sum(both(x2, 0), 0, xr2.at[0], x_right)
    send_sum(both(x2, 1), 1, xr2.at[1], x_left)
    pair[1].wait_recv()
    pair[2].wait_recv()
    send_sum(both(xr, 1), 2, xrn.at[0, 1], x_right)
    send_sum(both(xl, 0), 3, xrn.at[1, 0], x_left)
    got_sum(0, xr2.at[0])
    send_sum(both(xr, 0) + xr2[0].astype(F32), 4, xrn.at[0, 0], x_right)
    got_sum(1, xr2.at[1])
    send_sum(both(xl, 1) + xr2[1].astype(F32), 5, xrn.at[1, 1], x_left)
    pair[3].wait_recv()
    got_sum(2, xrn.at[0, 1])
    got_sum(3, xrn.at[1, 0])
    got_sum(4, xrn.at[0, 0])
    got_sum(5, xrn.at[1, 1])
    for half in range(2):
        total = both(x, half) + xrn[0, half].astype(F32) + xrn[1, half].astype(F32)
        out[pl.ds(16 * half, 16), :] = total.astype(BF16)
    for copy in y_sent + pair + x_sent:
        copy.wait_send()

    for i in range(1, 4):
        left_up(hops - 1, i)
        left_down(hops - 1, i)


def solution(mesh):
    zn = mesh.shape["sp"] // Y

    def per_device(
        normed,
        query_weight,
        key_weight,
        value_weight,
        pool_in_weight,
        pool_weight,
        map_balance,
        head_gain,
        contrast_out_weight,
        pool_out_weight,
    ):
        vmem = pl.BlockSpec(memory_space=pltpu.VMEM)
        hbm = pl.BlockSpec(memory_space=pl.ANY)
        dma = pltpu.SemaphoreType.DMA
        V = pltpu.VMEM
        return pl.pallas_call(
            functools.partial(kernel, zn),
            out_shape=pltpu.VMEM(normed.shape, BF16),
            in_specs=[hbm] * 10,
            out_specs=vmem,
            scratch_shapes=[
                V((8, 2, 16, 2048), BF16),
                V((2048, 512), BF16),
                V((2048, 256), BF16),
                V((2048, 128), BF16),
                V((256, 2048), BF16),
                V((128, 2048), BF16),
                V((1, 128, 128), BF16),
                V((1, 256), F32),
                pltpu.SMEM((8,), F32),
                V((Y, X, 64, 256), BF16),
                V((zn, X, 64, 512), BF16),
                V((Y, 2, 256, 256), F32),
                V((Y, 2, 256, 128), F32),
                V((Y, 2, 256, 128), F32),
                V((256, 128), BF16),
                V((16, 128), BF16),
                V((272, 128), F32),
                V((256, 2048), F32),
                V((6, 128, 512), BF16),
                V((6, 8, 128), F32),
                V((2, 128, 512), BF16),
                V((2, 8, 128), F32),
                V((2, 2, 128, 512), BF16),
                V((2, 2, 8, 128), F32),
                V((256, 256), BF16),
                V((X, 2, 2, 16, 2048), BF16),
                V((X, 2, 16, 2048), BF16),
                V((6, 16, 2048), BF16),
                V((2, 16, 2048), BF16),
                V((2, 2, 16, 2048), BF16),
                dma((11,)),
                dma((14,)),
                dma((8, 2)),
                dma((2, X)),
                dma((2, X)),
                dma((zn, X)),
                dma((12,)),
                dma((Y, X)),
                dma((2,)),
                dma((6, 2)),
                dma((X,)),
                dma((6,)),
            ],
            compiler_params=pltpu.CompilerParams(
                collective_id=0, has_side_effects=True, vmem_limit_bytes=66900000
            ),
        )(
            normed,
            query_weight,
            key_weight,
            value_weight,
            pool_in_weight,
            pool_weight,
            map_balance,
            head_gain.reshape(1, -1),
            contrast_out_weight,
            pool_out_weight,
        )

    return jax.shard_map(
        per_device,
        mesh=mesh,
        in_specs=(
            P(("sp", "tp"), None),
            P(None, "tp"),
            P(None, "tp"),
            P(None, "tp"),
            P(None, "tp"),
            P("tp", None, None),
            P(),
            P(),
            P("tp", None),
            P("tp", None),
        ),
        out_specs=P(("sp", "tp"), None),
        check_vma=False,
    )
```

```python
import functools
import math

import jax
import jax.numpy as jnp
from jax import lax
from jax.experimental import pallas as pl
from jax.experimental.pallas import tpu as pltpu
from jax.sharding import PartitionSpec as P

MESH = pl.DeviceIdType.MESH
F32 = jnp.float32
BF16 = jnp.bfloat16
Y = 4
X = 4
NEG = -1e30
norm_epsilon = 1e-06


def kernel(
    zn,
    normed_h,
    wq_h,
    wk_h,
    wv_h,
    wp_h,
    pool_weight_h,
    balance_h,
    gain_h,
    cow_h,
    pow_h,
    out,
    xg,
    wkv,
    wq,
    wp,
    cow,
    pow_,
    pool_weight,
    gain,
    balance,
    q_all,
    kv_all,
    acc,
    m_s,
    l_s,
    pin,
    rim,
    ext,
    pool_part,
    ps,
    pst,
    r2,
    r2t,
    rn,
    rnt,
    co,
    part,
    pr,
    xs,
    xr2,
    xrn,
    w_sem,
    xg_send,
    xg_recv,
    up_send,
    dn_send,
    kv_recv,
    q_send,
    q_recv,
    h_sem,
    ps_recv,
    pr_recv,
    xs_recv,
):
    sp = lax.axis_index("sp")
    tp = lax.axis_index("tp")
    nsp = zn * Y
    z, y = sp // Y, sp % Y
    x, core = tp // 2, tp % 2
    hops = zn // 2

    def at(zz, yy, xx, cc):
        return {"sp": zz * Y + yy, "tp": xx * 2 + cc}

    partner = at(z, y, x, 1 - core)
    xr, xl = (x + 1) % X, (x + X - 1) % X
    x2 = (x + 2) % X
    yr, yl = (y + 1) % Y, (y + Y - 1) % Y
    y2 = (y + 2) % Y
    zu, zd = (z + 1) % zn, (z + zn - 1) % zn
    x_right, x_left = at(z, y, xr, core), at(z, y, xl, core)
    y_right, y_left = at(z, yr, x, core), at(z, yl, x, core)
    z_up, z_down = at(zu, y, x, core), at(zd, y, x, core)
    next_sp = {"sp": (sp + 1) % nsp, "tp": tp}
    prev_sp = {"sp": (sp + nsp - 1) % nsp, "tp": tp}

    weights = [
        pltpu.make_async_copy(src, dst, w_sem.at[i])
        for i, (src, dst) in enumerate(
            (
                (wk_h, wkv.at[:, pl.ds(0, 256)]),
                (wv_h, wkv.at[:, pl.ds(256, 256)]),
                (wq_h, wq),
                (wp_h, wp),
                (pow_h, pow_),
                (cow_h, cow),
                (pool_weight_h, pool_weight),
                (gain_h, gain),
                (balance_h, balance),
            )
        )
    ]
    rows_in = [
        pltpu.make_async_copy(
            normed_h.at[pl.ds(16 * half, 16)], xg.at[tp, half], w_sem.at[len(weights) + half]
        )
        for half in range(2)
    ]
    for copy in rows_in + weights:
        copy.start()
    barrier = pltpu.get_barrier_semaphore()
    peers = (partner, x_right, x_left, y_right, y_left, z_up, z_down, next_sp, prev_sp)
    for peer in peers:
        pl.semaphore_signal(barrier, inc=1, device_id=peer, device_id_type=MESH)
    for j in range(Y):
        for c in range(2):
            m_s[j, c] = jnp.full((256, 128), NEG, F32)
            l_s[j, c] = jnp.zeros((256, 128), F32)
            acc[j, c] = jnp.zeros((256, 256), F32)
    pl.semaphore_wait(barrier, len(peers))
    for copy in rows_in:
        copy.wait()

    def remote(src, dst, send, recv, device):
        return pltpu.make_async_remote_copy(
            src_ref=src,
            dst_ref=dst,
            send_sem=send,
            recv_sem=recv,
            device_id=device,
            device_id_type=MESH,
        )
    sent = []

    def send_x(src, slot, half, device):
        copy = remote(src, xg.at[slot, half], xg_send.at[len(sent)], xg_recv.at[slot, half], device)
        copy.start()
        sent.append(copy)

    def got_x(slot, half):
        remote(
            xg.at[slot, half],
            xg.at[slot, half],
            xg_send.at[0],
            xg_recv.at[slot, half],
            partner,
        ).wait_recv()

    def own(half):
        return xg.at[tp, half]

    send_x(own(0), tp, 0, x_right)
    send_x(own(1), tp, 1, x_left)
    send_x(own(0), tp, 0, partner)
    send_x(own(1), tp, 1, partner)
    send_x(own(1), tp, 1, x_right)
    send_x(own(0), tp, 0, x_left)

    order = (x, xl, xr, x2)

    def kv_copy(slot, i, hop, up):
        piece = kv_all.at[slot, order[i]]
        return remote(
            piece,
            piece,
            (up_send if up else dn_send).at[hop % 2, i],
            kv_recv.at[slot, i],
            z_up if up else z_down,
        )

    def sends(s, i):
        up = jnp.logical_and(s <= z, z < zn - 1)
        up = jnp.logical_and(up, s + 1 <= (hops if i < 2 else hops - 1))
        dn = (z + s) % zn <= (hops - 1 if i >= 2 else hops - 2)
        dn = jnp.logical_and(dn, s + 1 <= (hops if i >= 2 else hops - 1))
        return up, dn

    def left_up(s, i):
        @pl.when(sends(s, i)[0])
        def _():
            kv_copy(jnp.maximum(z - s, 0), i, s, True).wait_send()

    def left_down(s, i):
        @pl.when(sends(s, i)[1])
        def _():
            kv_copy((z + s) % zn, i, s, False).wait_send()

    def kv_start(s, i):
        up, dn = sends(s, i)

        @pl.when(up)
        def _():
            kv_copy(jnp.maximum(z - s, 0), i, s, True).start()

        @pl.when(dn)
        def _():
            kv_copy((z + s) % zn, i, s, False).start()

    def pass_up(s, i):
        here = jnp.logical_and(s <= z, s <= (hops if i < 2 else hops - 1))
        if not (isinstance(s, int) and s < 2):
            left_up(s - 2, i)

        @pl.when(here)
        def _():
            kv_copy(jnp.maximum(z - s, 0), i, 0, True).wait_recv()

        @pl.when(sends(s, i)[0])
        def _():
            kv_copy(jnp.maximum(z - s, 0), i, s, True).start()

    def pass_down(s, i):
        here = (z + s) % zn <= (hops - 1 if i >= 2 else hops - 2)
        here = jnp.logical_and(here, s <= (hops if i >= 2 else hops - 1))
        if not (isinstance(s, int) and s < 2):
            left_down(s - 2, i)

        @pl.when(here)
        def _():
            kv_copy((z + s) % zn, i, 0, False).wait_recv()

        @pl.when(sends(s, i)[1])
        def _():
            kv_copy((z + s) % zn, i, s, False).start()

    def pass_on(s, i):
        pass_up(s, i)
        pass_down(s, i)

    def project(rows, weight):
        return jnp.dot(rows, weight[...], preferred_element_type=F32).astype(BF16)

    def project_kv(i):
        chip = order[i]
        rows = xg[pl.ds(2 * chip, 2)].reshape(64, 2048)
        kv_all[z, chip] = project(rows, wkv)
        kv_start(0, i)

    q_sent = []

    def q_copy(slot, i, device, send):
        piece = q_all.at[slot, order[i]]
        return remote(piece, piece, q_send.at[send], q_recv.at[slot, i], device)

    def send_q(slot, i, device):
        copy = q_copy(slot, i, device, len(q_sent))
        copy.start()
        q_sent.append(copy)

    def got_q(slot, i):
        q_copy(slot, i, y_right, 0).wait_recv()

    def project_q(i):
        chip = order[i]
        rows = xg[pl.ds(2 * chip, 2)].reshape(64, 2048)
        q_all[y, chip] = project(rows, wq)
        send_q(y, i, y_right)
        send_q(y, i, y_left)

    def relay_q(i):
        if i % 2 == 0:
            got_q(yl, i)
            send_q(yl, i, y_right)
        else:
            got_q(yr, i)
            send_q(yr, i, y_left)

    from_left, from_right, from_far = 2 * xl + core, 2 * xr + core, 2 * x2 + core

    def got_chip(chip):
        for half in range(2):
            got_x(2 * chip + 1 - core, half)
    weights[0].wait()
    weights[1].wait()
    got_chip(x)
    project_kv(0)
    weights[2].wait()
    project_q(0)
    got_x(from_left, 0)
    send_x(xg.at[from_left, 0], from_left, 0, x_right)
    got_x(from_right, 1)
    send_x(xg.at[from_right, 1], from_right, 1, x_left)
    send_x(xg.at[from_left, 0], from_left, 0, partner)
    send_x(xg.at[from_right, 1], from_right, 1, partner)
    pass_on(1, 0)
    got_x(from_left, 1)
    send_x(xg.at[from_left, 1], from_left, 1, partner)
    got_x(from_right, 0)
    send_x(xg.at[from_right, 0], from_right, 0, partner)
    got_chip(xl)
    project_kv(1)
    got_x(from_far, 0)
    send_x(xg.at[from_far, 0], from_far, 0, partner)
    got_x(from_far, 1)
    send_x(xg.at[from_far, 1], from_far, 1, partner)
    project_q(1)
    got_chip(xr)
    project_kv(2)
    pass_on(2, 0)
    got_chip(x2)
    project_kv(3)
    project_q(2)
    project_q(3)
    pass_on(1, 1)

    whole_rows = xg[...].reshape(256, 2048)
    weights[3].wait()
    pin[...] = project(whole_rows, wp)
    halo = remote(pin.at[pl.ds(240, 16)], rim, h_sem.at[0], h_sem.at[1], next_sp)
    halo.start()
    factor = 128 ** (-0.5) * math.log2(math.e)

    def attend(j, slot, masked):
        for c in range(2):
            cols = slice(128 * c, 128 * c + 128)
            q = q_all[j].reshape(256, 256)[:, cols]
            k = kv_all[slot].reshape(256, 512)[:, cols]
            v = kv_all[slot].reshape(256, 512)[:, 256:]
            s = lax.dot_general(q, k, (((1,), (1,)), ((), ())), preferred_element_type=F32) * factor
            if masked:
                row = lax.broadcasted_iota(jnp.int32, (256, 256), 0)
                col = lax.broadcasted_iota(jnp.int32, (256, 256), 1)
                s = jnp.where(col <= row, s, NEG)
            before = m_s[j, c]
            peak = jnp.maximum(before, jnp.max(s, axis=1, keepdims=True))
            shrink = jnp.exp2(before - peak)
            p = jnp.exp2(s - jnp.concatenate([peak, peak], axis=1))
            m_s[j, c] = peak
            l_s[j, c] = l_s[j, c] * shrink + (p[:, :128] + p[:, 128:])
            pv = jnp.dot(p.astype(BF16), v, preferred_element_type=F32)
            acc[j, c] = acc[j, c] * jnp.concatenate([shrink, shrink], axis=1) + pv

    partners = (y2, yr, yl, y)

    def work(u, group):
        s = u // 2 + 1
        up = u % 2 == 0
        slot = jnp.where(up, jnp.maximum(z - s, 0), (z + s) % zn)
        below = jnp.logical_and(up, s <= z)
        above = jnp.logical_and(z + s >= zn, jnp.logical_and(s < hops, jnp.logical_not(up)))

        @pl.when(jnp.logical_or(below, above))
        def _():
            for j in group:
                attend(j, slot, False)

    def work_once(done, ready):
        @pl.when(done < ready)
        def _():
            work(done, partners)

        return jnp.minimum(done + 1, ready)

    def pooling():
        halo.wait()
        ext[pl.ds(0, 16), :] = jnp.where(sp > 0, rim[...].astype(F32), 0.0)
        ext[pl.ds(16, 256), :] = pin[...].astype(F32)
        width = jnp.left_shift(jnp.int32(2), tp % 4)
        window = jnp.zeros((256, 128), F32)
        for offset in range(16):
            window = window + jnp.where(offset < width, ext[pl.ds(16 - offset, 256), :], 0.0)
        position = sp * 256 + lax.broadcasted_iota(jnp.int32, (256, 128), 0)
        counts = jnp.minimum(position + 1, width).astype(F32)
        spread = (window / counts - ext[pl.ds(16, 256), :]).astype(BF16)
        weights[6].wait()
        pool_out = jnp.dot(spread, pool_weight[0], preferred_element_type=F32).astype(BF16)
        weights[4].wait()
        for n in range(8):
            cols = slice(256 * n, 256 * n + 256)
            pool_part[:, cols] = jnp.dot(pool_out, pow_[:, cols], preferred_element_type=F32)
        for copy in weights[5:]:
            if copy is not weights[6]:
                copy.wait()
    relay_q(0)
    relay_q(1)
    attend(y, z, True)
    pass_on(1, 2)
    relay_q(2)
    relay_q(3)
    pass_on(3, 0)
    pass_on(1, 3)
    for i in range(4):
        if i % 2 == 0:
            got_q(yr, i)
        else:
            got_q(yl, i)
    for i in range(4):
        got_q(y2, i)
    pass_down(2, 1)
    pass_down(2, 2)

    def own_step(j, carry):
        @pl.when(j > y)
        def _():
            attend(j, z, False)

        return carry

    def ring_step(s, done):
        pass_up(s, 1)
        pass_down(s, 3)
        @pl.when(s == 2)
        def _():
            lax.fori_loop(0, Y, own_step, 0)

        done = work_once(done, jnp.where(s == 2, 0, 2 * (s - 1)))
        pass_on(s + 2, 0)
        done = work_once(done, 2 * (s - 1))
        pass_up(s, 2)
        pass_down(s + 1, 1)
        done = work_once(done, 2 * (s - 1))

        @pl.when(s == hops // 2 + 1)
        def _():
            pooling()
        pass_up(s, 3)
        pass_down(s + 1, 2)
        return done

    done = lax.fori_loop(2, hops, ring_step, 0)
    for copy in sent + q_sent:
        copy.wait_send()
    done = work_once(done, 2 * (hops - 1))
    done = work_once(done, 2 * (hops - 1))
    for i in (1, 2, 3):
        pass_up(hops, i)
    done = lax.fori_loop(
        done, 2 * (hops - 1), lambda i, d: work_once(d, 2 * (hops - 1)), done
    )
    pass_down(hops, 3)
    def state(j, half):
        rows = pl.ds(128 * half, 128)
        return [
            (
                m_s[j, c, rows, :],
                jnp.broadcast_to(jnp.sum(l_s[j, c, rows, :], axis=1, keepdims=True), (128, 128)),
                acc[j, c, rows, :],
            )
            for c in range(2)
        ]

    def arrived(payload, stats):
        columns = jnp.concatenate([stats[...], jnp.zeros((120, 128), F32)], axis=0).T
        return [
            (
                jnp.broadcast_to(columns[:, 2 * c : 2 * c + 1], (128, 128)),
                jnp.broadcast_to(columns[:, 2 * c + 1 : 2 * c + 2], (128, 128)),
                payload[:, 256 * c : 256 * c + 256].astype(F32),
            )
            for c in range(2)
        ]

    def joined(first, second):
        result = []
        for (m1, l1, a1), (m2, l2, a2) in zip(first, second):
            peak = jnp.maximum(m1, m2)
            s1, s2 = jnp.exp2(m1 - peak), jnp.exp2(m2 - peak)
            wide1 = jnp.concatenate([s1, s1], axis=1)
            wide2 = jnp.concatenate([s2, s2], axis=1)
            result.append((peak, l1 * s1 + l2 * s2, a1 * wide1 + a2 * wide2))
        return result

    y_sent = []

    def send_state(values, index, payload, stats, device):
        (m0, l0, a0), (m1, l1, a1) = values
        lane = lax.broadcasted_iota(jnp.int32, (128, 128), 1)
        table = jnp.where(lane == 0, m0, jnp.where(lane == 1, l0, jnp.where(lane == 2, m1, l1)))
        pst[index] = table.T[:8]
        ps[index, :, :256] = a0.astype(BF16)
        ps[index, :, 256:] = a1.astype(BF16)
        for i, (src, dst) in enumerate(((ps, payload), (pst, stats))):
            copy = remote(src.at[index], dst, q_send.at[2 * index + i], ps_recv.at[index, i], device)
            copy.start()
            y_sent.append(copy)

    def got_state(index, payload, stats):
        for i, (src, dst) in enumerate(((ps, payload), (pst, stats))):
            remote(
                src.at[index], dst, q_send.at[2 * index + i], ps_recv.at[index, i], y_right
            ).wait_recv()

    base = 2 * (hops - 1)
    work(base, (y2,))
    send_state(state(y2, 0), 0, r2.at[0], r2t.at[0], y_right)
    send_state(state(y2, 1), 1, r2.at[1], r2t.at[1], y_left)
    work(base, (yr, yl, y))
    send_state(state(yr, 1), 2, rn.at[0, 1], rnt.at[0, 1], y_right)
    send_state(state(yl, 0), 3, rn.at[1, 0], rnt.at[1, 0], y_left)
    got_state(0, r2.at[0], r2t.at[0])
    send_state(
        joined(state(yr, 0), arrived(r2.at[0], r2t.at[0])), 4, rn.at[0, 0], rnt.at[0, 0], y_right
    )
    got_state(1, r2.at[1], r2t.at[1])
    send_state(
        joined(state(yl, 1), arrived(r2.at[1], r2t.at[1])), 5, rn.at[1, 1], rnt.at[1, 1], y_left
    )
    level = balance[tp]
    got_state(2, rn.at[0, 1], rnt.at[0, 1])
    got_state(3, rn.at[1, 0], rnt.at[1, 0])
    for half in range(2):
        if half == 0:
            got_state(4, rn.at[0, 0], rnt.at[0, 0])
        else:
            got_state(5, rn.at[1, 1], rnt.at[1, 1])
        whole = state(y, half)
        for side in range(2):
            whole = joined(whole, arrived(rn.at[side, half], rnt.at[side, half]))
        maps = [
            (a / jnp.concatenate([l, l], axis=1)).astype(BF16).astype(F32) for _, l, a in whole
        ]
        contrast = maps[0] - level * maps[1]
        square = jnp.mean(contrast * contrast, axis=1, keepdims=True)
        contrast = contrast * lax.rsqrt(square + norm_epsilon) * gain[...]
        co[pl.ds(128 * half, 128), :] = contrast.astype(BF16)
    mixed = co[...]
    for n in range(8):
        cols = slice(256 * n, 256 * n + 256)
        tile = jnp.dot(mixed, cow[:, cols], preferred_element_type=F32) + pool_part[:, cols]
        part[:, :, :, :, cols] = tile.astype(BF16).reshape(X, 2, 2, 16, 256)
    pair = [
        remote(
            part.at[chip, 1 - core], pr.at[chip], xg_send.at[6 + i], pr_recv.at[i], partner
        )
        for i, chip in enumerate((x2, xr, xl, x))
    ]
    for copy in pair:
        copy.start()
    pair[0].wait_recv()
    def both(owner, half):
        return part[owner, core, half].astype(F32) + pr[owner, half].astype(F32)

    x_sent = []

    def send_sum(value, index, dst, device):
        xs[index] = value.astype(BF16)
        copy = remote(xs.at[index], dst, xg_send.at[index], xs_recv.at[index], device)
        copy.start()
        x_sent.append(copy)

    def got_sum(index, dst):
        remote(xs.at[index], dst, xg_send.at[index], xs_recv.at[index], x_right).wait_recv()

    send_sum(both(x2, 0), 0, xr2.at[0], x_right)
    send_sum(both(x2, 1), 1, xr2.at[1], x_left)
    pair[1].wait_recv()
    pair[2].wait_recv()
    send_sum(both(xr, 1), 2, xrn.at[0, 1], x_right)
    send_sum(both(xl, 0), 3, xrn.at[1, 0], x_left)
    got_sum(0, xr2.at[0])
    send_sum(both(xr, 0) + xr2[0].astype(F32), 4, xrn.at[0, 0], x_right)
    got_sum(1, xr2.at[1])
    send_sum(both(xl, 1) + xr2[1].astype(F32), 5, xrn.at[1, 1], x_left)
    pair[3].wait_recv()
    got_sum(2, xrn.at[0, 1])
    got_sum(3, xrn.at[1, 0])
    got_sum(4, xrn.at[0, 0])
    got_sum(5, xrn.at[1, 1])
    for half in range(2):
        total = both(x, half) + xrn[0, half].astype(F32) + xrn[1, half].astype(F32)
        out[pl.ds(16 * half, 16), :] = total.astype(BF16)
    for copy in y_sent + pair + x_sent:
        copy.wait_send()

    for i in range(1, 4):
        left_up(hops - 1, i)
        left_down(hops - 1, i)


def solution(mesh):
    zn = mesh.shape["sp"] // Y

    def per_device(
        normed,
        query_weight,
        key_weight,
        value_weight,
        pool_in_weight,
        pool_weight,
        map_balance,
        head_gain,
        contrast_out_weight,
        pool_out_weight,
    ):
        vmem = pl.BlockSpec(memory_space=pltpu.VMEM)
        hbm = pl.BlockSpec(memory_space=pl.ANY)
        dma = pltpu.SemaphoreType.DMA
        V = pltpu.VMEM
        return pl.pallas_call(
            functools.partial(kernel, zn),
            out_shape=pltpu.VMEM(normed.shape, BF16),
            in_specs=[hbm] * 10,
            out_specs=vmem,
            scratch_shapes=[
                V((8, 2, 16, 2048), BF16),
                V((2048, 512), BF16),
                V((2048, 256), BF16),
                V((2048, 128), BF16),
                V((256, 2048), BF16),
                V((128, 2048), BF16),
                V((1, 128, 128), BF16),
                V((1, 256), F32),
                pltpu.SMEM((8,), F32),
                V((Y, X, 64, 256), BF16),
                V((zn, X, 64, 512), BF16),
                V((Y, 2, 256, 256), F32),
                V((Y, 2, 256, 128), F32),
                V((Y, 2, 256, 128), F32),
                V((256, 128), BF16),
                V((16, 128), BF16),
                V((272, 128), F32),
                V((256, 2048), F32),
                V((6, 128, 512), BF16),
                V((6, 8, 128), F32),
                V((2, 128, 512), BF16),
                V((2, 8, 128), F32),
                V((2, 2, 128, 512), BF16),
                V((2, 2, 8, 128), F32),
                V((256, 256), BF16),
                V((X, 2, 2, 16, 2048), BF16),
                V((X, 2, 16, 2048), BF16),
                V((6, 16, 2048), BF16),
                V((2, 16, 2048), BF16),
                V((2, 2, 16, 2048), BF16),
                dma((11,)),
                dma((14,)),
                dma((8, 2)),
                dma((2, X)),
                dma((2, X)),
                dma((zn, X)),
                dma((12,)),
                dma((Y, X)),
                dma((2,)),
                dma((6, 2)),
                dma((X,)),
                dma((6,)),
            ],
            compiler_params=pltpu.CompilerParams(
                collective_id=0, has_side_effects=True, vmem_limit_bytes=66900000
            ),
        )(
            normed,
            query_weight,
            key_weight,
            value_weight,
            pool_in_weight,
            pool_weight,
            map_balance,
            head_gain.reshape(1, -1),
            contrast_out_weight,
            pool_out_weight,
        )

    return jax.shard_map(
        per_device,
        mesh=mesh,
        in_specs=(
            P(("sp", "tp"), None),
            P(None, "tp"),
            P(None, "tp"),
            P(None, "tp"),
            P(None, "tp"),
            P("tp", None, None),
            P(),
            P(),
            P("tp", None),
            P("tp", None),
        ),
        out_specs=P(("sp", "tp"), None),
        check_vma=False,
    )
```
